32 devices in a mesh: sp: 8 (over z, core), tp: 4 (over y, x).
Axes of the slice: x: 2, y: 2, z: 4, core: 2. Of those that a mesh axis runs over, the one named last changes fastest.
Arguments:
- residual: bfloat16 [3072, 2048], P('sp', 'tp'), may hold values from -40 to 40
- norm_gain: bfloat16 [3, 2048], P(None, 'tp'), may hold values from 0.099609375 to 1.8984375
- w_query: bfloat16 [3, 2048, 2048], P(None, 'tp'), may hold values from -2 to 2
- w_key: bfloat16 [3, 2048, 2048], P(None, 'tp'), may hold values from -8 to 8
- w_value: bfloat16 [3, 2048, 2048], P(None, 'tp'), may hold values from -0.125 to 0.125
- w_out: bfloat16 [3, 2048, 2048], P(None, 'tp'), may hold values from -0.25 to 0.25
- offset_bias: float32 [3, 32, 15, 31], P(None, 'tp'), may hold values from -5 to 5
Outputs:
- out_residual: bfloat16 [3072, 2048], P('sp', 'tp')
The draws below stay inside these ranges and needn't reach their ends.
All inputs are finite; a program needn't handle non-finite values.
Results may differ from the reference program's by a relative error of at most 0.014.
Values may be sent and summed in bfloat16 or wider, within the bound.
A program may use at most 128 MiB of HBM per device.

```python
import math
import jax
import jax.numpy as jnp
from jax import lax

D = 2048
HEADS = 32
HEAD_DIM = 64
GRID_W = 64
NA_ROWS = 8
NA_COLS = 16
LAYERS = 3
NA_W = 2048
ROWS = 48
TOKENS = 3072


def draw_residual(key, part):
    key_one, key_two = jax.random.split(jax.random.fold_in(key, 3), 2)
    ramp = jnp.arange(D, dtype=jnp.float32) / max(D - 1, 1)
    col_scale = jnp.exp(math.log(6.0) * ramp) / 2.5 * jnp.exp(jax.random.uniform(key_two, (D,), jnp.float32, -0.7, 0.7))
    values = jnp.clip(jax.random.normal(key_one, (TOKENS, D), jnp.float32), -4.0, 4.0)
    result = values * col_scale
    return result.astype(jnp.bfloat16)


def query_key_pair(key):
    key_query, key_key = jax.random.split(jax.random.fold_in(key, 11), 2)
    std = D ** (-0.5)
    query_w = jnp.clip(jax.random.normal(key_query, (LAYERS, NA_W, D), jnp.float32), -5.0, 5.0) * std
    key_w = jnp.clip(jax.random.normal(key_key, (LAYERS, NA_W, D), jnp.float32), -5.0, 5.0) * std
    return (query_w, key_w)


def draw_w_query(key, part):
    return query_key_pair(key)[0].astype(jnp.bfloat16)


def draw_w_key(key, part):
    return query_key_pair(key)[1].astype(jnp.bfloat16)


def block_scale(rng, extent, shards, smallest, largest):
    gain = 1.0
    for axis_at, parts in shards:
        draws = jax.random.uniform(jax.random.fold_in(jax.random.fold_in(rng, 6), axis_at), (parts,), jnp.float32, smallest / len(shards), largest / len(shards))
        gain = gain * jnp.repeat(jnp.exp(draws), extent[axis_at] // parts).reshape((-1,) + (1,) * (len(extent) - 1 - axis_at))
    return gain


def gaussian(rng, shape, scale, limit, shards=(), kind=jnp.bfloat16):
    drawn = jax.random.normal(rng, shape, jnp.float32) * scale
    if len(shards) > 0:
        drawn = block_scale(rng, shape, shards, -0.22, 0.18) * drawn
    return jnp.clip(drawn, min=-limit, max=limit).astype(kind)


def setup_inputs(seed: int = 0) -> dict:
    seeds = jax.random.split(jax.random.key(seed), 8)
    return {
        "residual": draw_residual(jax.random.fold_in(seeds[7], 71), 0),
        "norm_gain": jnp.clip(1.0 + 0.18 * jax.random.normal(seeds[1], (LAYERS, D), jnp.float32), 0.099609375, 1.8984375).astype(jnp.bfloat16),
        "w_query": draw_w_query(jax.random.fold_in(seeds[7], 71), 0),
        "w_key": draw_w_key(jax.random.fold_in(seeds[7], 71), 0),
        "w_value": gaussian(seeds[4], (LAYERS, NA_W, D), D ** -0.5, 0.125, ((1, 4),)),
        "w_out": gaussian(seeds[5], (LAYERS, D, NA_W), (NA_W // 4) ** -0.5, 0.25, ((1, 4),)),
        "offset_bias": gaussian(seeds[6], (LAYERS, HEADS, 2 * NA_ROWS - 1, 2 * NA_COLS - 1), 1.0, 5.0, ((1, 4),), jnp.float32),
    }


epsilon = 1e-06

def attend(queries, keys, values, lookup):
    rows_all = ROWS
    query_grid = queries.reshape(rows_all, GRID_W, HEADS, HEAD_DIM)
    key_grid = keys.reshape(rows_all, GRID_W, HEADS, HEAD_DIM)
    value_grid = values.reshape(rows_all, GRID_W, HEADS, HEAD_DIM)
    columns = jnp.arange(GRID_W, dtype=jnp.int32)
    col_index = jnp.clip(columns - NA_COLS // 2, 0, GRID_W - NA_COLS)[:, None] + jnp.arange(NA_COLS, dtype=jnp.int32)
    col_offset = col_index - columns[:, None] + (NA_COLS - 1)

    def row_block(row_global):
        first_row = jnp.clip(row_global - NA_ROWS // 2, 0, rows_all - NA_ROWS).astype(jnp.int32)
        query_row = lax.dynamic_index_in_dim(query_grid, row_global, 0, keepdims=False).astype(jnp.float32)
        key_window = lax.dynamic_slice_in_dim(key_grid, first_row, NA_ROWS, 0)[:, col_index].astype(jnp.float32)
        value_window = lax.dynamic_slice_in_dim(value_grid, first_row, NA_ROWS, 0)[:, col_index].astype(jnp.float32)
        row_offset = first_row + jnp.arange(NA_ROWS, dtype=jnp.int32) - row_global + (NA_ROWS - 1)
        bias_terms = lookup[:, row_offset[:, None, None], col_offset[None, :, :]].transpose(0, 2, 1, 3)
        scores = jnp.einsum('whd,rwkhd->hwrk', query_row, key_window) * HEAD_DIM ** (-0.5) + bias_terms
        weights = jax.nn.softmax(scores.reshape(HEADS, GRID_W, NA_ROWS * NA_COLS), axis=-1).astype(jnp.bfloat16)
        weights = lax.optimization_barrier(weights).astype(jnp.float32).reshape(HEADS, GRID_W, NA_ROWS, NA_COLS)
        attended = jnp.einsum('hwrk,rwkhd->whd', weights, value_window)
        return attended.astype(jnp.bfloat16).reshape(GRID_W, NA_W)
    return lax.map(row_block, jnp.arange(rows_all, dtype=jnp.int32)).reshape(rows_all * GRID_W, NA_W)

def reference(residual, norm_gain, w_query, w_key, w_value, w_out, offset_bias):
    stream = residual
    for layer_index in range(LAYERS):
        res_float = stream.astype(jnp.float32)
        mean_square = lax.optimization_barrier(jnp.mean(res_float * res_float, axis=1, keepdims=True))
        normed = (res_float * lax.rsqrt(mean_square + epsilon) * norm_gain[layer_index].astype(jnp.float32)).astype(jnp.bfloat16)
        queries = jnp.dot(normed, w_query[layer_index].T, preferred_element_type=jnp.float32).astype(jnp.bfloat16)
        keys = jnp.dot(normed, w_key[layer_index].T, preferred_element_type=jnp.float32).astype(jnp.bfloat16)
        values = jnp.dot(normed, w_value[layer_index].T, preferred_element_type=jnp.float32).astype(jnp.bfloat16)
        queries, keys, values = lax.optimization_barrier((queries, keys, values))
        attended = attend(queries, keys, values, offset_bias[layer_index])
        mixed = jnp.dot(attended, w_out[layer_index].T, preferred_element_type=jnp.float32)
        stream = (res_float + mixed).astype(jnp.bfloat16)
    return stream
```

```python
import jax
import jax.numpy as jnp
from jax import lax
from jax.experimental import pallas as pl
from jax.experimental.pallas import tpu as pltpu
from jax.sharding import PartitionSpec as P

HEAD_DIM = 64
GRID_W = 64
NA_ROWS = 8
NA_COLS = 16
LAYERS = 3


epsilon = 1e-06


def padded_2(array, sides, width):
    for axis, dim in sides:
        size, length = (lax.axis_size(axis), array.shape[dim])
        up = [(i, (i + 1) % size) for i in range(size - 1)]
        down = [(j, i) for i, j in up]
        last = lax.slice_in_dim(array, length - width, length, axis=dim)
        first = lax.slice_in_dim(array, 0, width, axis=dim)
        before = lax.ppermute(last, axis, up)
        after = lax.ppermute(first, axis, down)
        array = jnp.concatenate([before, array, after], axis=dim)
    return array


def shortened(array):
    return jax.tree.map(lambda a: a.astype(jnp.bfloat16) if a.dtype == jnp.float32 else a, array)


def contract(left, right):
    return lax.dot_general(
        left, right, (((1,), (1,)), ((), ())), preferred_element_type=jnp.float32
    )


def generic_device(residual, norm_gain, w_query, w_key, w_value, w_out, offset_bias):
    token_count = residual.shape[0]
    local_feats = residual.shape[1]
    local_heads = offset_bias.shape[1]
    head_cols = local_heads * HEAD_DIM
    rows_dev = token_count // GRID_W
    rows_all = rows_dev * lax.axis_size("sp")
    row_base = lax.axis_index("sp") * rows_dev
    reach = NA_ROWS // 2
    slab_width = min(2 * NA_COLS, GRID_W)
    tile_starts = list(range(0, GRID_W, NA_COLS))
    slab_starts = [min(max(start - NA_COLS // 2, 0), GRID_W - slab_width) for start in tile_starts]
    tile_info = []
    for start, slab in zip(tile_starts, slab_starts):
        query_cols = start + jnp.arange(NA_COLS, dtype=jnp.int32)
        key_cols = slab + jnp.arange(slab_width, dtype=jnp.int32)
        first_col = jnp.clip(query_cols - NA_COLS // 2, 0, GRID_W - NA_COLS)
        inside = (key_cols[None, :] >= first_col[:, None]) & (
            key_cols[None, :] < first_col[:, None] + NA_COLS
        )
        offsets = key_cols[None, :] - query_cols[:, None] + (NA_COLS - 1)
        onehot = (offsets[:, :, None] == jnp.arange(2 * NA_COLS - 1, dtype=jnp.int32)).astype(
            jnp.float32
        )
        tile_info.append((start, slab, inside, onehot))
    stream = residual
    for layer_index in range(LAYERS):
        res_float = stream.astype(jnp.float32)
        gathered, gain_all = (
            lax.all_gather(stream, "tp", axis=1, tiled=True),
            lax.all_gather(norm_gain[layer_index][None, :], "tp", axis=1, tiled=True),
        )
        full_float = gathered.astype(jnp.float32)
        inverse = lax.rsqrt(jnp.mean(full_float * full_float, axis=1, keepdims=True) + epsilon)
        normed_all = (full_float * inverse * gain_all.astype(jnp.float32)).astype(jnp.bfloat16)
        queries = contract(normed_all, w_query[layer_index])
        keys = contract(normed_all, w_key[layer_index])
        values = contract(normed_all, w_value[layer_index])
        queries = queries.astype(jnp.bfloat16)
        key_value = jnp.concatenate(
            [keys.astype(jnp.bfloat16), values.astype(jnp.bfloat16)], axis=1
        )
        padded = padded_2(key_value, (("sp", 0),), reach * GRID_W)
        key_grid = padded.reshape(rows_dev + 2 * reach, GRID_W, 2, local_heads, HEAD_DIM)
        query_grid = queries.reshape(rows_dev, GRID_W, local_heads, HEAD_DIM)
        lookup = offset_bias[layer_index]

        def one_row(row_index, query_row):
            row_global = row_base + row_index
            first_row = jnp.clip(row_global - reach, 0, rows_all - NA_ROWS)
            local_first = first_row - row_base + reach
            window = lax.dynamic_slice_in_dim(key_grid, local_first, NA_ROWS, 0)
            row_offset = (
                first_row + jnp.arange(NA_ROWS, dtype=jnp.int32) - row_global + (NA_ROWS - 1)
            )
            row_onehot = (
                row_offset[:, None] == jnp.arange(2 * NA_ROWS - 1, dtype=jnp.int32)
            ).astype(jnp.float32)
            row_bias = jnp.einsum(
                "hab,ra->hrb", lookup, row_onehot, precision=lax.Precision.HIGHEST
            )
            pieces = []
            for start, slab, inside, onehot in tile_info:
                query_tile = query_row[start : start + NA_COLS]
                slab_keys = window[:, slab : slab + slab_width, 0]
                slab_values = window[:, slab : slab + slab_width, 1]
                bias_terms = jnp.einsum(
                    "hrb,wsb->hwrs", row_bias, onehot, precision=lax.Precision.HIGHEST
                )
                scores = jnp.einsum(
                    "whd,rshd->hwrs", query_tile, slab_keys, preferred_element_type=jnp.float32
                )
                scores = scores * HEAD_DIM ** (-0.5) + bias_terms
                scores = jnp.where(inside[None, :, None, :], scores, -jnp.inf)
                weights = jax.nn.softmax(
                    scores.reshape(local_heads, NA_COLS, NA_ROWS * slab_width), axis=-1
                ).astype(jnp.bfloat16)
                weights = weights.reshape(local_heads, NA_COLS, NA_ROWS, slab_width)
                attended = jnp.einsum(
                    "hwrs,rshd->whd", weights, slab_values, preferred_element_type=jnp.float32
                )
                pieces.append(attended.astype(jnp.bfloat16).reshape(NA_COLS, head_cols))
            return jnp.concatenate(pieces, axis=0)

        attended = jax.vmap(one_row)(jnp.arange(rows_dev, dtype=jnp.int32), query_grid).reshape(
            token_count, head_cols
        )
        portion = jax.tree.map(
            lambda part: lax.all_gather(part, "tp", axis=1, tiled=True), shortened(attended)
        )
        out_rows = lax.slice_in_dim(w_out[layer_index], 0, portion.shape[1], axis=1)
        mixed = jnp.zeros((token_count, local_feats), jnp.float32) + contract(portion, out_rows)
        stream = (res_float + mixed).astype(jnp.bfloat16)
    return stream


def window_mask():
    shape = (GRID_W, 2 * GRID_W)
    key_col = lax.broadcasted_iota(jnp.int32, shape, 0)
    query_col = lax.broadcasted_iota(jnp.int32, shape, 1) % GRID_W
    first = jnp.clip(query_col - NA_COLS // 2, 0, GRID_W - NA_COLS)
    return (key_col >= first) & (key_col < first + NA_COLS)


def flip_matrix(count, base):
    shape = (count, 2 * GRID_W)
    source = lax.broadcasted_iota(jnp.int32, shape, 0)
    lane = lax.broadcasted_iota(jnp.int32, shape, 1)
    return (lane == base + count - 1 - source).astype(jnp.float32)


def pair_lanes(bias):
    row_offs, heads, col_offs = bias.shape
    flat = bias.reshape(row_offs * heads, col_offs)
    low, high = (
        jnp.dot(
            flat,
            flip_matrix(col_offs, base),
            precision=lax.Precision.HIGHEST,
            preferred_element_type=jnp.float32,
        )
        for base in (0, GRID_W)
    )
    return low, high


def build_table(lanes_of, table):
    inside = window_mask()
    for off in range(2 * NA_ROWS - 1):
        row = jnp.broadcast_to(lanes_of(off), (GRID_W, 2 * GRID_W))
        rolled = pltpu.roll(row, 2 * GRID_W - (NA_COLS - 1), axis=1, stride=1, stride_axis=0)
        table[off * GRID_W : (off + 1) * GRID_W, :] = jnp.where(inside, rolled, -1e30)


def attend_row(query, window_keys, window_values, bias):
    low = lax.broadcasted_iota(jnp.int32, query.shape, 1) < HEAD_DIM
    zero = jnp.zeros_like(query)
    block = jnp.concatenate([jnp.where(low, query, zero), jnp.where(low, zero, query)], axis=0)
    scores = contract(window_keys, block) + bias
    top = jnp.max(scores, axis=0, keepdims=True)
    weights = jnp.exp(scores - top)
    inverse = 1.0 / jnp.sum(weights, axis=0, keepdims=True)
    weights = (weights * inverse).astype(jnp.bfloat16)
    mixed = lax.dot_general(
        weights, window_values, (((0,), (0,)), ((), ())), preferred_element_type=jnp.float32
    )
    return jnp.where(low, mixed[:GRID_W], mixed[GRID_W:]).astype(jnp.bfloat16)


MESH = pl.DeviceIdType.MESH
REACH = NA_ROWS // 2
UP, DOWN = REACH, NA_ROWS - REACH - 1
AHEAD = 4
PERIOD = 16
FINISH, ATTEND, RELAY, LAST = 2, 6, 11, 13
TALL = 2 * GRID_W


def tp_copy(src, dst, sems, index, peer):
    return pltpu.make_async_remote_copy(
        src_ref=src,
        dst_ref=dst,
        send_sem=sems.at[0, index],
        recv_sem=sems.at[1, index],
        device_id=(lax.axis_index("sp"), peer),
        device_id_type=MESH,
    )


class SquareGather:
    def __init__(self, slots, sems, row_of):
        self.slots, self.sems, self.row_of = slots, sems, row_of
        self.me = lax.axis_index("tp")
        self.across = self.me + 1 - 2 * (self.me % 2)
        self.over = (self.me + 2) % 4
        self.corner = (self.across + 2) % 4

    def copy(self, kind, slot, index, peer):
        start, size = self.row_of(index) * GRID_W, GRID_W
        if kind >= 2:
            size = GRID_W // 2
            start = start + (kind - 2) * size
        part = self.slots.at[slot, pl.ds(pl.multiple_of(start, size), size), :]
        return tp_copy(part, part, self.sems.at[kind], index, peer)

    def send(self, index):
        self.copy(0, self.me, index, self.across).start()
        self.copy(1, self.me, index, self.over).start()

    def relay(self, index):
        self.copy(0, self.across, index, self.across).wait_recv()
        self.copy(2, self.across, index, self.over).start()
        self.copy(1, self.over, index, self.over).wait_recv()
        self.copy(3, self.over, index, self.across).start()

    def finish(self, index):
        self.copy(2, self.corner, index, self.over).wait_recv()
        self.copy(3, self.corner, index, self.across).wait_recv()

    def drain(self, index):
        self.copy(0, self.me, index, self.across).wait_send()
        self.copy(1, self.me, index, self.over).wait_send()
        self.copy(2, self.across, index, self.over).wait_send()
        self.copy(3, self.over, index, self.across).wait_send()


def halo_needs(rows_dev, sp_size):
    rows_all = rows_dev * sp_size
    picks = {"first": 0, "last": sp_size - 1}
    if sp_size > 2:
        picks.update(even=2, odd=1)
    needs = {}
    for kind, sp in picks.items():
        base, seen, steps = sp * rows_dev, set(), []
        for index in range(rows_dev):
            row = base + (rows_dev - 1 - index if sp % 2 else index)
            start = min(max(row - REACH, 0), rows_all - NA_ROWS)
            window = range(start, start + NA_ROWS)
            new = [(True, k) for k in range(UP) if base - UP + k in window]
            new += [(False, k) for k in range(DOWN) if base + rows_dev + k in window]
            steps.append([need for need in new if need not in seen])
            seen.update(new)
        for k in range(UP):
            if sp > 0 and (True, k) not in seen:
                steps[-1].append((True, k))
        for k in range(DOWN):
            if sp < sp_size - 1 and (False, k) not in seen:
                steps[-1].append((False, k))
        needs[kind] = steps
    return needs


def stack_kernel(
    rows_dev, needs,
    x_ref, gain_ref, bias_ref, wq_ref, wk_ref, wv_ref, wo_ref, out_ref,
    gains, weights, stream, mixed, keyval, queries, scaled, squares, sums, tables, bias, partial,
    weight_sems, gain_sems, stream_sems, mixed_sems, halo_sems, local_sems,
):
    sp, sp_size = lax.axis_index("sp"), lax.axis_size("sp")
    layers = wq_ref.shape[0]
    tokens, feats = x_ref.shape
    width, total_feats = feats, 4 * feats
    odd = sp % 2

    def row_of(index):
        return index + odd * (rows_dev - 1 - 2 * index)

    streams = SquareGather(stream, stream_sems, row_of)
    mixes = SquareGather(mixed, mixed_sems, row_of)
    me, across, over, corner = streams.me, streams.across, streams.over, streams.corner
    sources = (wk_ref, wv_ref, wq_ref, wo_ref)

    def rows_at(row):
        return pl.ds(pl.multiple_of(row * GRID_W, GRID_W), GRID_W)

    def pair_at(index):
        low = jnp.minimum(row_of(index), row_of(index - 1))
        return pl.ds(pl.multiple_of(low * GRID_W, TALL), TALL)

    def weight_copy(kind, layer):
        return pltpu.make_async_copy(
            sources[kind].at[layer], weights.at[kind, layer], weight_sems.at[kind, layer]
        )

    load_x = pltpu.make_async_copy(x_ref, stream.at[me], local_sems.at[rows_dev])
    load_bias = pltpu.make_async_copy(bias_ref, bias, local_sems.at[rows_dev + 1])
    load_x.start()
    load_bias.start()

    barrier = pltpu.get_barrier_semaphore()
    for peer in (across, over, corner):
        pl.semaphore_signal(barrier, inc=1, device_id=(sp, peer), device_id_type=MESH)

    @pl.when(sp > 0)
    def _():
        pl.semaphore_signal(barrier, inc=1, device_id=(sp - 1, me), device_id_type=MESH)

    @pl.when(sp < sp_size - 1)
    def _():
        pl.semaphore_signal(barrier, inc=1, device_id=(sp + 1, me), device_id_type=MESH)

    for layer in range(layers):
        for kind in range(4):
            weight_copy(kind, layer).start()

    gains[me, 0:layers, :] = gain_ref[...].astype(jnp.float32)
    sides = jnp.minimum(sp, 1) + jnp.minimum(sp_size - 1 - sp, 1)
    load_x.wait()
    pl.semaphore_wait(barrier, 3 + sides)

    def gain_copy(index, slot, peer):
        return tp_copy(gains.at[slot], gains.at[slot], gain_sems, index, peer)

    for index, peer in enumerate((across, over, corner)):
        gain_copy(index, me, peer).start()
    for index in range(AHEAD):
        streams.send(index)

    def halo_copy(parity, up, k):
        local = rows_dev - UP + k if up else k
        there = k if up else UP + rows_dev + k
        return pltpu.make_async_remote_copy(
            src_ref=keyval.at[parity, rows_at(UP + local), :],
            dst_ref=keyval.at[parity, rows_at(there), :],
            send_sem=halo_sems.at[0, parity, int(up), k],
            recv_sem=halo_sems.at[1, parity, int(up), k],
            device_id=(sp + 1 if up else sp - 1, me),
            device_id_type=MESH,
        )

    def project(layer, slot, kind, source):
        cols = pl.ds(pl.multiple_of(slot * width, width), width)
        return contract(source, weights[kind, layer, :, cols])

    def scale_slot(layer, slot, here):
        part = stream[slot, here, :].astype(jnp.float32)
        square = part * part
        folded = square[:, :128]
        for start in range(128, feats, 128):
            folded += square[:, start : start + 128]
        return (part * gains[slot, pl.ds(layer, 1), :]).astype(jnp.bfloat16), folded

    def drain_mixed(index):
        for row in range(AHEAD - 1, rows_dev):

            @pl.when(index == row)
            def _(row=row):
                last = rows_dev if row == rows_dev - 1 else row - DOWN + 1
                for done in range(row - DOWN, last):
                    mixes.drain(done)

    def relay_stream(layer, index):
        @pl.when((layer == 0) & (index == 0))
        def _():
            load_bias.wait()
            for place, peer in enumerate((across, over, corner)):
                gain_copy(place, peer, peer).wait_recv()
                gain_copy(place, me, peer).wait_send()

        streams.relay(index)

        @pl.when((layer == 0) & (index + AHEAD < rows_dev))
        def _():
            streams.send(index + AHEAD)

        @pl.when(index == 0)
        def _():
            for kind in range(3):
                weight_copy(kind, layer).wait()

    def start_pair(layer, index):
        here, turn = pair_at(index), index // 2 % 2
        folded = jnp.zeros((TALL, 128), jnp.float32)
        for place, slot in enumerate((me, across, over)):
            scaled[place], square = scale_slot(layer, slot, here)
            folded += square
        squares[turn] = folded
        for kind in range(3):
            total = project(layer, me, kind, scaled[0])
            total += project(layer, across, kind, scaled[1])
            sums[turn, kind] = total + project(layer, over, kind, scaled[2])

    def end_pair(layer, index):
        here, turn, parity = pair_at(index), index // 2 % 2, layer % 2
        streams.finish(index - 1)
        streams.finish(index)
        source, folded = scale_slot(layer, corner, here)
        total = jnp.sum(squares[turn] + folded, axis=1, keepdims=True)
        inverse = lax.rsqrt(total * (1.0 / total_feats) + epsilon)
        there = pl.ds(pl.multiple_of(here.start + UP * GRID_W, GRID_W), TALL)
        for kind in range(2):
            keyval[parity, there, kind * width : (kind + 1) * width] = (
                (sums[turn, kind] + project(layer, corner, kind, source)) * inverse
            ).astype(jnp.bfloat16)
        for row in (row_of(index - 1), row_of(index)):

            @pl.when((row < DOWN) & (sp > 0))
            def _(row=row):
                halo_copy(parity, False, row).start()

            @pl.when((row >= rows_dev - UP) & (sp < sp_size - 1))
            def _(row=row):
                halo_copy(parity, True, row - (rows_dev - UP)).start()

        queries[here, :] = (
            (sums[turn, 2] + project(layer, corner, 2, source)) * inverse
        ).astype(jnp.bfloat16) * jnp.bfloat16(HEAD_DIM ** (-0.5))

    def make_tables(layer, index):
        @pl.when(index == 0)
        def _():
            low, high = pair_lanes(bias[layer])
            heads = bias.shape[2]

            def lanes_of(pair):
                def at(off):
                    place = off * heads + 2 * pair
                    return low[place : place + 1] + high[place + 1 : place + 2]

                return at

            for pair in range(width // 128):
                build_table(lanes_of(pair), tables.at[pair])

    kinds = {
        "first": sp == 0,
        "last": sp == sp_size - 1,
        "even": (odd == 0) & (sp > 0),
        "odd": (odd == 1) & (sp < sp_size - 1),
    }

    def wait_halo(parity, index):
        for kind, steps in needs.items():
            for step, rows in enumerate(steps):
                if rows:

                    @pl.when(kinds[kind] & (index == step))
                    def _(rows=rows):
                        for up, k in rows:
                            halo_copy(parity, up, k).wait_recv()

    def attend(layer, index):
        row, parity = row_of(index), layer % 2
        here = rows_at(row)
        wait_halo(parity, index)
        base = sp * rows_dev
        first = jnp.clip(base + row - REACH, 0, rows_dev * sp_size - NA_ROWS)
        start, off = first - base + UP, first - base - row + NA_ROWS - 1
        keys = pl.ds(pl.multiple_of(start * GRID_W, GRID_W), NA_ROWS * GRID_W)
        offs = pl.ds(pl.multiple_of(off * GRID_W, GRID_W), NA_ROWS * GRID_W)
        for pair in range(width // 128):
            cols = slice(pair * 128, (pair + 1) * 128)
            vcols = slice(width + pair * 128, width + (pair + 1) * 128)
            mixed[me, here, cols] = attend_row(
                queries[here, cols],
                keyval[parity, keys, cols],
                keyval[parity, keys, vcols],
                tables[pair, offs, :],
            )
        streams.drain(index)
        mixes.send(index)

        @pl.when(index == rows_dev - 1)
        def _():
            @pl.when(sp > 0)
            def _():
                for k in range(DOWN):
                    halo_copy(parity, False, k).wait_send()

            @pl.when(sp < sp_size - 1)
            def _():
                for k in range(UP):
                    halo_copy(parity, True, k).wait_send()

    def relay_mixed(layer, index):
        mixes.relay(index)

        @pl.when(index == 0)
        def _():
            weight_copy(3, layer).wait()

    def start_mixed(layer, index):
        here = pair_at(index)
        total = stream[me, here, :].astype(jnp.float32)
        for slot in (me, across, over):
            total += project(layer, slot, 3, mixed[slot, here, :])
        partial[index // 2 % 2] = total

    def store_out(index):
        here = pair_at(index)
        return pltpu.make_async_copy(
            stream.at[me, here, :], out_ref.at[here, :], local_sems.at[index]
        )

    def end_mixed(layer, index):
        here = pair_at(index)
        mixes.finish(index - 1)
        mixes.finish(index)
        total = partial[index // 2 % 2] + project(layer, corner, 3, mixed[corner, here, :])
        stream[me, here, :] = total.astype(jnp.bfloat16)

        @pl.when(layer < layers - 1)
        def _():
            for row in (index - 1, index):
                drain_mixed(row)
                streams.send(row)

        @pl.when(layer == layers - 1)
        def _():
            store_out(index).start()

    early = (odd == 0) & (sp > 0)
    steps = (
        (relay_mixed, RELAY, 1),
        (start_mixed, RELAY, 2),
        (end_mixed, LAST, 2),
        (relay_stream, 0, 1),
        (end_pair, FINISH, 2),
        (start_pair, 0, 2),
        (make_tables, 0, 1),
        (attend, ATTEND + 1 - early.astype(jnp.int32), 1),
    )

    def tick(now, carry):
        for step, delay, rows in steps:
            since = now - delay

            @pl.when((since >= 0) & (since < layers * PERIOD))
            def _(step=step, since=since, rows=rows):
                layer, index = since // PERIOD, since % PERIOD

                @pl.when((index < rows_dev) & (index % rows == rows - 1))
                def _():
                    step(layer, index)

        return carry

    lax.fori_loop(0, PERIOD * (layers - 1) + LAST + rows_dev, tick, 0)
    for index in range(rows_dev):
        mixes.drain(index)
    for index in range(1, rows_dev, 2):
        store_out(index).wait()


def square_device(residual, norm_gain, w_query, w_key, w_value, w_out, offset_bias):
    tokens, feats = residual.shape
    layers, heads, row_offs, col_offs = offset_bias.shape
    rows_dev = tokens // GRID_W
    vmem = pl.BlockSpec(memory_space=pltpu.VMEM)
    hbm = pl.BlockSpec(memory_space=pl.ANY)
    bf16, f32, dma = jnp.bfloat16, jnp.float32, pltpu.SemaphoreType.DMA
    padded = tokens + (UP + DOWN) * GRID_W
    needs = halo_needs(rows_dev, lax.axis_size("sp"))
    return pl.pallas_call(
        lambda *refs: stack_kernel(rows_dev, needs, *refs),
        out_shape=jax.ShapeDtypeStruct(residual.shape, bf16),
        in_specs=[hbm, vmem] + [hbm] * 5,
        out_specs=hbm,
        scratch_shapes=[
            pltpu.VMEM((4, -(-layers // 8) * 8, feats), f32),
            pltpu.VMEM((4,) + w_query.shape, bf16),
            pltpu.VMEM((4, tokens, feats), bf16),
            pltpu.VMEM((4, tokens, feats), bf16),
            pltpu.VMEM((2, padded, 2 * feats), bf16),
            pltpu.VMEM((tokens, feats), bf16),
            pltpu.VMEM((3, TALL, feats), bf16),
            pltpu.VMEM((2, TALL, 128), f32),
            pltpu.VMEM((2, 3, TALL, feats), f32),
            pltpu.VMEM((feats // 128, row_offs * GRID_W, 128), f32),
            pltpu.VMEM((layers, row_offs, heads, col_offs), f32),
            pltpu.VMEM((2, TALL, feats), f32),
            dma((4, layers)),
            dma((2, 3)),
            dma((4, 2, rows_dev)),
            dma((4, 2, rows_dev)),
            dma((2, 2, 2, max(UP, DOWN))),
            dma((rows_dev + 2,)),
        ],
        compiler_params=pltpu.CompilerParams(
            collective_id=0, has_side_effects=True, vmem_limit_bytes=56 * 1024 * 1024
        ),
        name="stack",
    )(residual, norm_gain, offset_bias.transpose(0, 2, 1, 3), w_query, w_key, w_value, w_out)


def per_device(residual, norm_gain, w_query, w_key, w_value, w_out, offset_bias):
    paired = offset_bias.shape[1] % 8 == 0 and 2 * HEAD_DIM == 128 and 2 * GRID_W == 128
    square = lax.axis_size("tp") == 4 and offset_bias.shape[1] * HEAD_DIM == residual.shape[1]
    rows_dev = residual.shape[0] // GRID_W
    even = lax.axis_size("sp") % 2 == 0 and rows_dev == ATTEND
    body = generic_device
    if paired and square and even:
        body = square_device
    return body(residual, norm_gain, w_query, w_key, w_value, w_out, offset_bias)


def solution(mesh):
    in_specs = (
        P("sp", "tp"),
        P(None, "tp"),
        P(None, "tp", None),
        P(None, "tp", None),
        P(None, "tp", None),
        P(None, "tp", None),
        P(None, "tp", None, None),
    )
    out_specs = P("sp", "tp")
    return jax.shard_map(
        per_device, mesh=mesh, in_specs=in_specs, out_specs=out_specs, check_vma=False
    )
```

```python
import jax
import jax.numpy as jnp
from jax import lax
from jax.experimental import pallas as pl
from jax.experimental.pallas import tpu as pltpu
from jax.sharding import PartitionSpec as P

HEAD_DIM = 64
GRID_W = 64
NA_ROWS = 8
NA_COLS = 16
LAYERS = 3


epsilon = 1e-06


def padded_2(array, sides, width):
    for axis, dim in sides:
        size, length = (lax.axis_size(axis), array.shape[dim])
        up = [(i, (i + 1) % size) for i in range(size - 1)]
        down = [(j, i) for i, j in up]
        last = lax.slice_in_dim(array, length - width, length, axis=dim)
        first = lax.slice_in_dim(array, 0, width, axis=dim)
        before = lax.ppermute(last, axis, up)
        after = lax.ppermute(first, axis, down)
        array = jnp.concatenate([before, array, after], axis=dim)
    return array


def shortened(array):
    return jax.tree.map(lambda a: a.astype(jnp.bfloat16) if a.dtype == jnp.float32 else a, array)


def contract(left, right):
    return lax.dot_general(
        left, right, (((1,), (1,)), ((), ())), preferred_element_type=jnp.float32
    )


def generic_device(residual, norm_gain, w_query, w_key, w_value, w_out, offset_bias):
    token_count = residual.shape[0]
    local_feats = residual.shape[1]
    local_heads = offset_bias.shape[1]
    head_cols = local_heads * HEAD_DIM
    rows_dev = token_count // GRID_W
    rows_all = rows_dev * lax.axis_size("sp")
    row_base = lax.axis_index("sp") * rows_dev
    reach = NA_ROWS // 2
    slab_width = min(2 * NA_COLS, GRID_W)
    tile_starts = list(range(0, GRID_W, NA_COLS))
    slab_starts = [min(max(start - NA_COLS // 2, 0), GRID_W - slab_width) for start in tile_starts]
    tile_info = []
    for start, slab in zip(tile_starts, slab_starts):
        query_cols = start + jnp.arange(NA_COLS, dtype=jnp.int32)
        key_cols = slab + jnp.arange(slab_width, dtype=jnp.int32)
        first_col = jnp.clip(query_cols - NA_COLS // 2, 0, GRID_W - NA_COLS)
        inside = (key_cols[None, :] >= first_col[:, None]) & (
            key_cols[None, :] < first_col[:, None] + NA_COLS
        )
        offsets = key_cols[None, :] - query_cols[:, None] + (NA_COLS - 1)
        onehot = (offsets[:, :, None] == jnp.arange(2 * NA_COLS - 1, dtype=jnp.int32)).astype(
            jnp.float32
        )
        tile_info.append((start, slab, inside, onehot))
    stream = residual
    for layer_index in range(LAYERS):
        res_float = stream.astype(jnp.float32)
        gathered, gain_all = (
            lax.all_gather(stream, "tp", axis=1, tiled=True),
            lax.all_gather(norm_gain[layer_index][None, :], "tp", axis=1, tiled=True),
        )
        full_float = gathered.astype(jnp.float32)
        inverse = lax.rsqrt(jnp.mean(full_float * full_float, axis=1, keepdims=True) + epsilon)
        normed_all = (full_float * inverse * gain_all.astype(jnp.float32)).astype(jnp.bfloat16)
        queries = contract(normed_all, w_query[layer_index])
        keys = contract(normed_all, w_key[layer_index])
        values = contract(normed_all, w_value[layer_index])
        queries = queries.astype(jnp.bfloat16)
        key_value = jnp.concatenate(
            [keys.astype(jnp.bfloat16), values.astype(jnp.bfloat16)], axis=1
        )
        padded = padded_2(key_value, (("sp", 0),), reach * GRID_W)
        key_grid = padded.reshape(rows_dev + 2 * reach, GRID_W, 2, local_heads, HEAD_DIM)
        query_grid = queries.reshape(rows_dev, GRID_W, local_heads, HEAD_DIM)
        lookup = offset_bias[layer_index]

        def one_row(row_index, query_row):
            row_global = row_base + row_index
            first_row = jnp.clip(row_global - reach, 0, rows_all - NA_ROWS)
            local_first = first_row - row_base + reach
            window = lax.dynamic_slice_in_dim(key_grid, local_first, NA_ROWS, 0)
            row_offset = (
                first_row + jnp.arange(NA_ROWS, dtype=jnp.int32) - row_global + (NA_ROWS - 1)
            )
            row_onehot = (
                row_offset[:, None] == jnp.arange(2 * NA_ROWS - 1, dtype=jnp.int32)
            ).astype(jnp.float32)
            row_bias = jnp.einsum(
                "hab,ra->hrb", lookup, row_onehot, precision=lax.Precision.HIGHEST
            )
            pieces = []
            for start, slab, inside, onehot in tile_info:
                query_tile = query_row[start : start + NA_COLS]
                slab_keys = window[:, slab : slab + slab_width, 0]
                slab_values = window[:, slab : slab + slab_width, 1]
                bias_terms = jnp.einsum(
                    "hrb,wsb->hwrs", row_bias, onehot, precision=lax.Precision.HIGHEST
                )
                scores = jnp.einsum(
                    "whd,rshd->hwrs", query_tile, slab_keys, preferred_element_type=jnp.float32
                )
                scores = scores * HEAD_DIM ** (-0.5) + bias_terms
                scores = jnp.where(inside[None, :, None, :], scores, -jnp.inf)
                weights = jax.nn.softmax(
                    scores.reshape(local_heads, NA_COLS, NA_ROWS * slab_width), axis=-1
                ).astype(jnp.bfloat16)
                weights = weights.reshape(local_heads, NA_COLS, NA_ROWS, slab_width)
                attended = jnp.einsum(
                    "hwrs,rshd->whd", weights, slab_values, preferred_element_type=jnp.float32
                )
                pieces.append(attended.astype(jnp.bfloat16).reshape(NA_COLS, head_cols))
            return jnp.concatenate(pieces, axis=0)

        attended = jax.vmap(one_row)(jnp.arange(rows_dev, dtype=jnp.int32), query_grid).reshape(
            token_count, head_cols
        )
        portion = jax.tree.map(
            lambda part: lax.all_gather(part, "tp", axis=1, tiled=True), shortened(attended)
        )
        out_rows = lax.slice_in_dim(w_out[layer_index], 0, portion.shape[1], axis=1)
        mixed = jnp.zeros((token_count, local_feats), jnp.float32) + contract(portion, out_rows)
        stream = (res_float + mixed).astype(jnp.bfloat16)
    return stream


def window_mask():
    shape = (GRID_W, 2 * GRID_W)
    key_col = lax.broadcasted_iota(jnp.int32, shape, 0)
    query_col = lax.broadcasted_iota(jnp.int32, shape, 1) % GRID_W
    first = jnp.clip(query_col - NA_COLS // 2, 0, GRID_W - NA_COLS)
    return (key_col >= first) & (key_col < first + NA_COLS)


def flip_matrix(count, base):
    shape = (count, 2 * GRID_W)
    source = lax.broadcasted_iota(jnp.int32, shape, 0)
    lane = lax.broadcasted_iota(jnp.int32, shape, 1)
    return (lane == base + count - 1 - source).astype(jnp.float32)


def pair_lanes(bias):
    row_offs, heads, col_offs = bias.shape
    flat = bias.reshape(row_offs * heads, col_offs)
    low, high = (
        jnp.dot(
            flat,
            flip_matrix(col_offs, base),
            precision=lax.Precision.HIGHEST,
            preferred_element_type=jnp.float32,
        )
        for base in (0, GRID_W)
    )
    return low, high


def build_table(lanes_of, table):
    inside = window_mask()
    for off in range(2 * NA_ROWS - 1):
        row = jnp.broadcast_to(lanes_of(off), (GRID_W, 2 * GRID_W))
        rolled = pltpu.roll(row, 2 * GRID_W - (NA_COLS - 1), axis=1, stride=1, stride_axis=0)
        table[off * GRID_W : (off + 1) * GRID_W, :] = jnp.where(inside, rolled * LOG2E, -1e30)


def attend_row(query, window_keys, window_values, bias):
    low = lax.broadcasted_iota(jnp.int32, query.shape, 1) < HEAD_DIM
    zero = jnp.zeros_like(query)
    block = jnp.concatenate([jnp.where(low, query, zero), jnp.where(low, zero, query)], axis=0)
    scores = contract(window_keys, block) + bias
    weights = jnp.exp2(scores - jnp.max(scores, axis=0, keepdims=True)).astype(jnp.bfloat16)
    ones = jnp.ones_like(window_values)
    mixed = lax.dot_general(
        weights, jnp.concatenate([window_values, ones], axis=1), (((0,), (0,)), ((), ())),
        preferred_element_type=jnp.float32,
    )
    mixed = mixed[:, : 2 * HEAD_DIM] / mixed[:, 2 * HEAD_DIM :]
    return jnp.where(low, mixed[:GRID_W], mixed[GRID_W:]).astype(jnp.bfloat16)


MESH = pl.DeviceIdType.MESH
LOG2E = 1.4426950408889634
REACH = NA_ROWS // 2
UP, DOWN = REACH, NA_ROWS - REACH - 1
AHEAD = 4
TALL = 2 * GRID_W


def tp_copy(src, dst, sems, index, peer):
    return pltpu.make_async_remote_copy(
        src_ref=src,
        dst_ref=dst,
        send_sem=sems.at[0, index],
        recv_sem=sems.at[1, index],
        device_id=(lax.axis_index("sp"), peer),
        device_id_type=MESH,
    )


class SquareGather:
    def __init__(self, slots, sems, row_of, halves):
        self.slots, self.sems, self.row_of, self.halves = slots, sems, row_of, halves
        self.me = lax.axis_index("tp")
        self.across = self.me + 1 - 2 * (self.me % 2)
        self.over = (self.me + 2) % 4
        self.corner = (self.across + 2) % 4

    def copy(self, kind, slot, index, half, peer):
        start = pl.multiple_of(self.row_of(index) * GRID_W, GRID_W)
        width = self.slots.shape[2]
        if kind == 2 or self.halves == 2:
            width = width // 2
        cols = slice(half * width, (half + 1) * width)
        part = self.slots.at[slot, pl.ds(start, GRID_W), cols]
        return tp_copy(part, part, self.sems.at[kind], 2 * index + half, peer)

    def send(self, index, half=0):
        self.copy(0, self.me, index, half, self.across).start()
        self.copy(1, self.me, index, half, self.over).start()

    def relay(self, index, half):
        take = half if self.halves == 2 else 0
        if half == 0:
            self.copy(0, self.across, index, take, self.across).wait_recv()
            self.copy(2, self.across, index, half, self.over).start()
        else:
            self.copy(1, self.over, index, take, self.over).wait_recv()
            self.copy(2, self.over, index, half, self.across).start()

    def settle(self, index):
        self.copy(0, self.across, index, 1, self.across).wait_recv()
        self.copy(1, self.over, index, 0, self.over).wait_recv()

    def finish(self, index):
        self.copy(2, self.corner, index, 0, self.over).wait_recv()
        self.copy(2, self.corner, index, 1, self.across).wait_recv()

    def drain(self, index):
        for half in range(self.halves):
            self.copy(0, self.me, index, half, self.across).wait_send()
            self.copy(1, self.me, index, half, self.over).wait_send()
        self.copy(2, self.across, index, 0, self.over).wait_send()
        self.copy(2, self.over, index, 1, self.across).wait_send()


def halo_needs(rows_dev, sp_size):
    rows_all = rows_dev * sp_size
    picks = {"first": 0, "last": sp_size - 1}
    if sp_size > 2:
        picks.update(even=2, odd=1)
    needs = {}
    for kind, sp in picks.items():
        base, seen, steps = sp * rows_dev, set(), []
        for index in range(rows_dev):
            row = base + (index if sp % 2 else rows_dev - 1 - index)
            start = min(max(row - REACH, 0), rows_all - NA_ROWS)
            window = range(start, start + NA_ROWS)
            new = [(True, k) for k in range(UP) if base - UP + k in window]
            new += [(False, k) for k in range(DOWN) if base + rows_dev + k in window]
            steps.append([need for need in new if need not in seen])
            seen.update(new)
        for k in range(UP):
            if sp > 0 and (True, k) not in seen:
                steps[-1].append((True, k))
        for k in range(DOWN):
            if sp < sp_size - 1 and (False, k) not in seen:
                steps[-1].append((False, k))
        needs[kind] = steps
    return needs


def stack_kernel(
    rows_dev, needs,
    x_ref, gain_ref, bias_ref, wq_ref, wk_ref, wv_ref, wo_ref, out_ref,
    gains, weights, stream, mixed, keyval, queries, scaled, squares, sums, tables, bias, partial,
    weight_sems, gain_sems, stream_sems, mixed_sems, halo_sems, local_sems,
):
    sp, sp_size = lax.axis_index("sp"), lax.axis_size("sp")
    layers = wq_ref.shape[0]
    tokens, feats = x_ref.shape
    width, total_feats = feats, 4 * feats
    even = 1 - sp % 2

    def row_of(index):
        return index + even * (rows_dev - 1 - 2 * index)

    streams = SquareGather(stream, stream_sems, row_of, 1)
    mixes = SquareGather(mixed, mixed_sems, row_of, 2)
    me, across, over, corner = streams.me, streams.across, streams.over, streams.corner
    sources = (wk_ref, wv_ref, wq_ref, wo_ref)

    def rows_at(row):
        return pl.ds(pl.multiple_of(row * GRID_W, GRID_W), GRID_W)

    def pair_at(chunk):
        low = jnp.minimum(row_of(2 * chunk), row_of(2 * chunk + 1))
        return pl.ds(pl.multiple_of(low * GRID_W, TALL), TALL)

    def weight_copy(kind, layer):
        return pltpu.make_async_copy(
            sources[kind].at[layer], weights.at[kind, layer], weight_sems.at[kind, layer]
        )

    load_x = pltpu.make_async_copy(x_ref, stream.at[me], local_sems.at[rows_dev])
    load_bias = pltpu.make_async_copy(bias_ref, bias, local_sems.at[rows_dev + 1])
    load_x.start()
    load_bias.start()

    barrier = pltpu.get_barrier_semaphore()
    for peer in (across, over, corner):
        pl.semaphore_signal(barrier, inc=1, device_id=(sp, peer), device_id_type=MESH)

    @pl.when(sp > 0)
    def _():
        pl.semaphore_signal(barrier, inc=1, device_id=(sp - 1, me), device_id_type=MESH)

    @pl.when(sp < sp_size - 1)
    def _():
        pl.semaphore_signal(barrier, inc=1, device_id=(sp + 1, me), device_id_type=MESH)

    for layer in range(layers):
        for kind in range(4):
            weight_copy(kind, layer).start()

    gains[me, 0:layers, :] = gain_ref[...].astype(jnp.float32)
    sides = jnp.minimum(sp, 1) + jnp.minimum(sp_size - 1 - sp, 1)
    load_x.wait()
    pl.semaphore_wait(barrier, 3 + sides)

    def gain_copy(index, slot, peer):
        return tp_copy(gains.at[slot], gains.at[slot], gain_sems, index, peer)

    for index, peer in enumerate((across, over, corner)):
        gain_copy(index, me, peer).start()
    for index in range(AHEAD):
        streams.send(index)

    def halo_copy(parity, up, k):
        local = rows_dev - UP + k if up else k
        there = k if up else UP + rows_dev + k
        return pltpu.make_async_remote_copy(
            src_ref=keyval.at[parity, rows_at(UP + local), :],
            dst_ref=keyval.at[parity, rows_at(there), :],
            send_sem=halo_sems.at[0, parity, int(up), k],
            recv_sem=halo_sems.at[1, parity, int(up), k],
            device_id=(sp + 1 if up else sp - 1, me),
            device_id_type=MESH,
        )

    def project(layer, slot, kind, source):
        cols = pl.ds(pl.multiple_of(slot * width, width), width)
        return contract(source, weights[kind, layer, :, cols])

    def scale_slot(layer, slot, here):
        part = stream[slot, here, :].astype(jnp.float32)
        square = part * part
        folded = square[:, :128]
        for start in range(128, feats, 128):
            folded += square[:, start : start + 128]
        return (part * gains[slot, pl.ds(layer, 1), :]).astype(jnp.bfloat16), folded

    def drain_mixed(row):
        if row >= DOWN:
            last = rows_dev if row == rows_dev - 1 else row - DOWN + 1
            for done in range(row - DOWN, last):
                mixes.drain(done)

    def relay_stream(layer, index):
        if index == 0:

            @pl.when(layer == 0)
            def _():
                for place, peer in enumerate((across, over, corner)):
                    gain_copy(place, peer, peer).wait_recv()
                    gain_copy(place, me, peer).wait_send()

        streams.relay(index, 0)
        streams.relay(index, 1)
        if index + AHEAD < rows_dev:

            @pl.when(layer == 0)
            def _():
                streams.send(index + AHEAD)

    def start_rows(layer, chunk, kind):
        here = pair_at(chunk)
        slots = (me, across, over)
        if kind == 0:
            folded = jnp.zeros((TALL, 128), jnp.float32)
            for place, slot in enumerate(slots):
                scaled[chunk, place], square = scale_slot(layer, slot, here)
                folded += square
            squares[chunk] = folded
        if chunk == 0:
            weight_copy(kind, layer).wait()
        sums[chunk, kind] = sum(
            project(layer, slot, kind, scaled[chunk, place]) for place, slot in enumerate(slots)
        )

    def end_rows(layer, chunk, part):
        here, parity = pair_at(chunk), layer % 2
        if part == 1:
            queries[here, :] = (
                (sums[chunk, 2] + project(layer, corner, 2, scaled[chunk, 3]))
                * (squares[chunk, :, :1] * (HEAD_DIM ** (-0.5) * LOG2E))
            ).astype(jnp.bfloat16)
            return
        rows = (2 * chunk, 2 * chunk + 1)
        for index in rows:
            streams.finish(index)
        source, folded = scale_slot(layer, corner, here)
        scaled[chunk, 3] = source
        total = jnp.sum(squares[chunk] + folded, axis=1, keepdims=True)
        inverse = lax.rsqrt(total * (1.0 / total_feats) + epsilon)
        squares[chunk] = jnp.broadcast_to(inverse, (TALL, 128))
        there = pl.ds(pl.multiple_of(here.start + UP * GRID_W, GRID_W), TALL)
        for kind in range(2):
            keyval[parity, there, kind * width : (kind + 1) * width] = (
                (sums[chunk, kind] + project(layer, corner, kind, source)) * inverse
            ).astype(jnp.bfloat16)
        for index in rows:
            row = row_of(index)

            @pl.when((row < DOWN) & (sp > 0))
            def _(row=row):
                halo_copy(parity, False, row).start()

            @pl.when((row >= rows_dev - UP) & (sp < sp_size - 1))
            def _(row=row):
                halo_copy(parity, True, row - (rows_dev - UP)).start()

    def make_tables(layer):
        @pl.when(layer == 0)
        def _():
            load_bias.wait()

        low, high = pair_lanes(bias[layer])
        heads = bias.shape[2]

        def lanes_of(pair):
            def at(off):
                place = off * heads + 2 * pair
                return low[place : place + 1] + high[place + 1 : place + 2]

            return at

        for pair in range(width // 128):
            build_table(lanes_of(pair), tables.at[pair])

    kinds = {
        "first": sp == 0,
        "last": sp == sp_size - 1,
        "even": (even == 1) & (sp > 0),
        "odd": (even == 0) & (sp < sp_size - 1),
    }
    early = kinds["odd"]

    def wait_halo(parity, index):
        for kind, steps in needs.items():
            if steps[index]:

                @pl.when(kinds[kind])
                def _(rows=steps[index]):
                    for up, k in rows:
                        halo_copy(parity, up, k).wait_recv()

    def attend(layer, index, half):
        row, parity = row_of(index), layer % 2
        here = rows_at(row)
        if half == 0:
            wait_halo(parity, index)
        base = sp * rows_dev
        first = jnp.clip(base + row - REACH, 0, rows_dev * sp_size - NA_ROWS)
        start, off = first - base + UP, first - base - row + NA_ROWS - 1
        keys = pl.ds(pl.multiple_of(start * GRID_W, GRID_W), NA_ROWS * GRID_W)
        offs = pl.ds(pl.multiple_of(off * GRID_W, GRID_W), NA_ROWS * GRID_W)
        pairs = width // 256
        for pair in range(half * pairs, (half + 1) * pairs):
            cols = slice(pair * 128, (pair + 1) * 128)
            vcols = slice(width + pair * 128, width + (pair + 1) * 128)
            mixed[me, here, cols] = attend_row(
                queries[here, cols],
                keyval[parity, keys, cols],
                keyval[parity, keys, vcols],
                tables[pair, offs, :],
            )
        if half == 1:
            streams.drain(index)
        mixes.send(index, half)
        if index == rows_dev - 1 and half == 1:

            @pl.when(sp > 0)
            def _():
                for k in range(DOWN):
                    halo_copy(parity, False, k).wait_send()

            @pl.when(sp < sp_size - 1)
            def _():
                for k in range(UP):
                    halo_copy(parity, True, k).wait_send()

    def relay_mixed(layer, index, half):
        mixes.relay(index, half)

    def start_mixed(layer, chunk):
        here = pair_at(chunk)
        for index in (2 * chunk, 2 * chunk + 1):
            mixes.settle(index)
        if chunk == 0:
            weight_copy(3, layer).wait()
        total = stream[me, here, :].astype(jnp.float32)
        for slot in (me, across, over):
            total += project(layer, slot, 3, mixed[slot, here, :])
        partial[chunk] = total

    def store_out(chunk):
        here = pair_at(chunk)
        return pltpu.make_async_copy(
            stream.at[me, here, :], out_ref.at[here, :], local_sems.at[chunk]
        )

    def end_mixed(layer, chunk):
        here = pair_at(chunk)
        rows = (2 * chunk, 2 * chunk + 1)
        for index in rows:
            mixes.finish(index)
        total = partial[chunk] + project(layer, corner, 3, mixed[corner, here, :])
        stream[me, here, :] = total.astype(jnp.bfloat16)

        @pl.when(layer < layers - 1)
        def _():
            for index in rows:
                drain_mixed(index)
                streams.send(index)

        @pl.when(layer == layers - 1)
        def _():
            store_out(chunk).start()

    plan = (
        (make_tables, None),
        (relay_stream, None, 0),
        (relay_stream, None, 1),
        (start_rows, None, 0, 0),
        (start_rows, None, 0, 1),
        (start_rows, None, 0, 2),
        (relay_stream, None, 2),
        (relay_stream, None, 3),
        (start_rows, None, 1, 0),
        (start_rows, None, 1, 1),
        (start_rows, None, 1, 2),
        (end_rows, None, 0, 0),
        (relay_stream, None, 4),
        (end_rows, None, 0, 1),
        (end_rows, None, 1, 0),
        (relay_stream, None, 5),
        (start_rows, None, 2, 0),
        (start_rows, None, 2, 1),
        (start_rows, None, 2, 2),
        (end_rows, None, 1, 1),
        (end_rows, None, 2, 0),
        (attend, early, 0, 0),
        (attend, early, 0, 1),
        (end_rows, None, 2, 1),
        (attend, ~early, 0, 0),
        (attend, ~early, 0, 1),
        (attend, None, 1, 0),
        (attend, None, 1, 1),
        (attend, None, 2, 0),
        (attend, None, 2, 1),
        (attend, ~early, 3, 0),
        (attend, ~early, 3, 1),
        (attend, ~early, 4, 0),
        (attend, ~early, 4, 1),
        (attend, ~early, 5, 0),
        (attend, ~early, 5, 1),
        (relay_mixed, None, 0, 0),
        (relay_mixed, None, 0, 1),
        (relay_mixed, None, 1, 0),
        (relay_mixed, None, 1, 1),
        (relay_mixed, None, 2, 0),
        (attend, early, 3, 0),
        (attend, early, 3, 1),
        (attend, early, 4, 0),
        (attend, early, 4, 1),
        (attend, early, 5, 0),
        (attend, early, 5, 1),
        (start_mixed, None, 0),
        (relay_mixed, None, 2, 1),
        (relay_mixed, None, 3, 0),
        (relay_mixed, None, 3, 1),
        (start_mixed, None, 1),
        (relay_mixed, None, 4, 0),
        (relay_mixed, None, 4, 1),
        (relay_mixed, None, 5, 0),
        (relay_mixed, None, 5, 1),
        (end_mixed, None, 0),
        (start_mixed, None, 2),
        (end_mixed, None, 1),
        (end_mixed, None, 2),
    )

    def one_layer(layer, carry):
        for step, when, *place in plan:
            if when is None:
                step(layer, *place)
            else:
                pl.when(when)(lambda: step(layer, *place))
        return carry

    lax.fori_loop(0, layers, one_layer, 0)
    for index in range(rows_dev):
        mixes.drain(index)
    for chunk in range(rows_dev // 2):
        store_out(chunk).wait()


def square_device(residual, norm_gain, w_query, w_key, w_value, w_out, offset_bias):
    tokens, feats = residual.shape
    layers, heads, row_offs, col_offs = offset_bias.shape
    rows_dev = tokens // GRID_W
    vmem = pl.BlockSpec(memory_space=pltpu.VMEM)
    hbm = pl.BlockSpec(memory_space=pl.ANY)
    bf16, f32, dma = jnp.bfloat16, jnp.float32, pltpu.SemaphoreType.DMA
    padded = tokens + (UP + DOWN) * GRID_W
    needs = halo_needs(rows_dev, lax.axis_size("sp"))
    return pl.pallas_call(
        lambda *refs: stack_kernel(rows_dev, needs, *refs),
        out_shape=jax.ShapeDtypeStruct(residual.shape, bf16),
        in_specs=[hbm, vmem] + [hbm] * 5,
        out_specs=hbm,
        scratch_shapes=[
            pltpu.VMEM((4, -(-layers // 8) * 8, feats), f32),
            pltpu.VMEM((4,) + w_query.shape, bf16),
            pltpu.VMEM((4, tokens, feats), bf16),
            pltpu.VMEM((4, tokens, feats), bf16),
            pltpu.VMEM((2, padded, 2 * feats), bf16),
            pltpu.VMEM((tokens, feats), bf16),
            pltpu.VMEM((rows_dev // 2, 4, TALL, feats), bf16),
            pltpu.VMEM((rows_dev // 2, TALL, 128), f32),
            pltpu.VMEM((rows_dev // 2, 3, TALL, feats), f32),
            pltpu.VMEM((feats // 128, row_offs * GRID_W, 128), f32),
            pltpu.VMEM((layers, row_offs, heads, col_offs), f32),
            pltpu.VMEM((rows_dev // 2, TALL, feats), f32),
            dma((4, layers)),
            dma((2, 3)),
            dma((3, 2, 2 * rows_dev)),
            dma((3, 2, 2 * rows_dev)),
            dma((2, 2, 2, max(UP, DOWN))),
            dma((rows_dev + 2,)),
        ],
        compiler_params=pltpu.CompilerParams(
            collective_id=0, has_side_effects=True, vmem_limit_bytes=56 * 1024 * 1024
        ),
        name="stack",
    )(residual, norm_gain, offset_bias.transpose(0, 2, 1, 3), w_query, w_key, w_value, w_out)


def per_device(residual, norm_gain, w_query, w_key, w_value, w_out, offset_bias):
    paired = offset_bias.shape[1] % 8 == 0 and 2 * HEAD_DIM == 128 and 2 * GRID_W == 128
    square = lax.axis_size("tp") == 4 and offset_bias.shape[1] * HEAD_DIM == residual.shape[1]
    rows_dev = residual.shape[0] // GRID_W
    even = lax.axis_size("sp") % 2 == 0 and rows_dev == 2 * (AHEAD - 1)
    body = generic_device
    if paired and square and even:
        body = square_device
    return body(residual, norm_gain, w_query, w_key, w_value, w_out, offset_bias)


def solution(mesh):
    in_specs = (
        P("sp", "tp"),
        P(None, "tp"),
        P(None, "tp", None),
        P(None, "tp", None),
        P(None, "tp", None),
        P(None, "tp", None),
        P(None, "tp", None, None),
    )
    out_specs = P("sp", "tp")
    return jax.shard_map(
        per_device, mesh=mesh, in_specs=in_specs, out_specs=out_specs, check_vma=False
    )
```

```python
import jax
import jax.numpy as jnp
from jax import lax
from jax.experimental import pallas as pl
from jax.experimental.pallas import tpu as pltpu
from jax.sharding import PartitionSpec as P

HEAD_DIM = 64
GRID_W = 64
NA_ROWS = 8
NA_COLS = 16
LAYERS = 3


epsilon = 1e-06


def padded_2(array, sides, width):
    for axis, dim in sides:
        size, length = (lax.axis_size(axis), array.shape[dim])
        up = [(i, (i + 1) % size) for i in range(size - 1)]
        down = [(j, i) for i, j in up]
        last = lax.slice_in_dim(array, length - width, length, axis=dim)
        first = lax.slice_in_dim(array, 0, width, axis=dim)
        before = lax.ppermute(last, axis, up)
        after = lax.ppermute(first, axis, down)
        array = jnp.concatenate([before, array, after], axis=dim)
    return array


def shortened(array):
    return jax.tree.map(lambda a: a.astype(jnp.bfloat16) if a.dtype == jnp.float32 else a, array)


def contract(left, right):
    return lax.dot_general(
        left, right, (((1,), (1,)), ((), ())), preferred_element_type=jnp.float32
    )


def generic_device(residual, norm_gain, w_query, w_key, w_value, w_out, offset_bias):
    token_count = residual.shape[0]
    local_feats = residual.shape[1]
    local_heads = offset_bias.shape[1]
    head_cols = local_heads * HEAD_DIM
    rows_dev = token_count // GRID_W
    rows_all = rows_dev * lax.axis_size("sp")
    row_base = lax.axis_index("sp") * rows_dev
    reach = NA_ROWS // 2
    slab_width = min(2 * NA_COLS, GRID_W)
    tile_starts = list(range(0, GRID_W, NA_COLS))
    slab_starts = [min(max(start - NA_COLS // 2, 0), GRID_W - slab_width) for start in tile_starts]
    tile_info = []
    for start, slab in zip(tile_starts, slab_starts):
        query_cols = start + jnp.arange(NA_COLS, dtype=jnp.int32)
        key_cols = slab + jnp.arange(slab_width, dtype=jnp.int32)
        first_col = jnp.clip(query_cols - NA_COLS // 2, 0, GRID_W - NA_COLS)
        inside = (key_cols[None, :] >= first_col[:, None]) & (
            key_cols[None, :] < first_col[:, None] + NA_COLS
        )
        offsets = key_cols[None, :] - query_cols[:, None] + (NA_COLS - 1)
        onehot = (offsets[:, :, None] == jnp.arange(2 * NA_COLS - 1, dtype=jnp.int32)).astype(
            jnp.float32
        )
        tile_info.append((start, slab, inside, onehot))
    stream = residual
    for layer_index in range(LAYERS):
        res_float = stream.astype(jnp.float32)
        gathered, gain_all = (
            lax.all_gather(stream, "tp", axis=1, tiled=True),
            lax.all_gather(norm_gain[layer_index][None, :], "tp", axis=1, tiled=True),
        )
        full_float = gathered.astype(jnp.float32)
        inverse = lax.rsqrt(jnp.mean(full_float * full_float, axis=1, keepdims=True) + epsilon)
        normed_all = (full_float * inverse * gain_all.astype(jnp.float32)).astype(jnp.bfloat16)
        queries = contract(normed_all, w_query[layer_index])
        keys = contract(normed_all, w_key[layer_index])
        values = contract(normed_all, w_value[layer_index])
        queries = queries.astype(jnp.bfloat16)
        key_value = jnp.concatenate(
            [keys.astype(jnp.bfloat16), values.astype(jnp.bfloat16)], axis=1
        )
        padded = padded_2(key_value, (("sp", 0),), reach * GRID_W)
        key_grid = padded.reshape(rows_dev + 2 * reach, GRID_W, 2, local_heads, HEAD_DIM)
        query_grid = queries.reshape(rows_dev, GRID_W, local_heads, HEAD_DIM)
        lookup = offset_bias[layer_index]

        def one_row(row_index, query_row):
            row_global = row_base + row_index
            first_row = jnp.clip(row_global - reach, 0, rows_all - NA_ROWS)
            local_first = first_row - row_base + reach
            window = lax.dynamic_slice_in_dim(key_grid, local_first, NA_ROWS, 0)
            row_offset = (
                first_row + jnp.arange(NA_ROWS, dtype=jnp.int32) - row_global + (NA_ROWS - 1)
            )
            row_onehot = (
                row_offset[:, None] == jnp.arange(2 * NA_ROWS - 1, dtype=jnp.int32)
            ).astype(jnp.float32)
            row_bias = jnp.einsum(
                "hab,ra->hrb", lookup, row_onehot, precision=lax.Precision.HIGHEST
            )
            pieces = []
            for start, slab, inside, onehot in tile_info:
                query_tile = query_row[start : start + NA_COLS]
                slab_keys = window[:, slab : slab + slab_width, 0]
                slab_values = window[:, slab : slab + slab_width, 1]
                bias_terms = jnp.einsum(
                    "hrb,wsb->hwrs", row_bias, onehot, precision=lax.Precision.HIGHEST
                )
                scores = jnp.einsum(
                    "whd,rshd->hwrs", query_tile, slab_keys, preferred_element_type=jnp.float32
                )
                scores = scores * HEAD_DIM ** (-0.5) + bias_terms
                scores = jnp.where(inside[None, :, None, :], scores, -jnp.inf)
                weights = jax.nn.softmax(
                    scores.reshape(local_heads, NA_COLS, NA_ROWS * slab_width), axis=-1
                ).astype(jnp.bfloat16)
                weights = weights.reshape(local_heads, NA_COLS, NA_ROWS, slab_width)
                attended = jnp.einsum(
                    "hwrs,rshd->whd", weights, slab_values, preferred_element_type=jnp.float32
                )
                pieces.append(attended.astype(jnp.bfloat16).reshape(NA_COLS, head_cols))
            return jnp.concatenate(pieces, axis=0)

        attended = jax.vmap(one_row)(jnp.arange(rows_dev, dtype=jnp.int32), query_grid).reshape(
            token_count, head_cols
        )
        portion = jax.tree.map(
            lambda part: lax.all_gather(part, "tp", axis=1, tiled=True), shortened(attended)
        )
        out_rows = lax.slice_in_dim(w_out[layer_index], 0, portion.shape[1], axis=1)
        mixed = jnp.zeros((token_count, local_feats), jnp.float32) + contract(portion, out_rows)
        stream = (res_float + mixed).astype(jnp.bfloat16)
    return stream


def window_mask():
    shape = (GRID_W, 2 * GRID_W)
    key_col = lax.broadcasted_iota(jnp.int32, shape, 0)
    query_col = lax.broadcasted_iota(jnp.int32, shape, 1) % GRID_W
    first = jnp.clip(query_col - NA_COLS // 2, 0, GRID_W - NA_COLS)
    return (key_col >= first) & (key_col < first + NA_COLS)


def flip_matrix(count, base):
    shape = (count, 2 * GRID_W)
    source = lax.broadcasted_iota(jnp.int32, shape, 0)
    lane = lax.broadcasted_iota(jnp.int32, shape, 1)
    return (lane == base + count - 1 - source).astype(jnp.float32)


def pair_lanes(bias):
    row_offs, heads, col_offs = bias.shape
    flat = bias.reshape(row_offs * heads, col_offs)
    low, high = (
        jnp.dot(
            flat,
            flip_matrix(col_offs, base),
            precision=lax.Precision.HIGHEST,
            preferred_element_type=jnp.float32,
        )
        for base in (0, GRID_W)
    )
    return low, high


def build_table(lanes_of, table):
    inside = window_mask()
    for off in range(2 * NA_ROWS - 1):
        row = jnp.broadcast_to(lanes_of(off), (GRID_W, 2 * GRID_W))
        rolled = pltpu.roll(row, 2 * GRID_W - (NA_COLS - 1), axis=1, stride=1, stride_axis=0)
        table[off * GRID_W : (off + 1) * GRID_W, :] = jnp.where(inside, rolled * LOG2E, -1e30)


def attend_row(query, window_keys, window_values, bias):
    low = lax.broadcasted_iota(jnp.int32, query.shape, 1) < HEAD_DIM
    zero = jnp.zeros_like(query)
    block = jnp.concatenate([jnp.where(low, query, zero), jnp.where(low, zero, query)], axis=0)
    scores = contract(window_keys, block) + bias
    weights = jnp.exp2(scores - jnp.max(scores, axis=0, keepdims=True)).astype(jnp.bfloat16)
    ones = jnp.ones_like(window_values)
    mixed = lax.dot_general(
        weights, jnp.concatenate([window_values, ones], axis=1), (((0,), (0,)), ((), ())),
        preferred_element_type=jnp.float32,
    )
    mixed = mixed[:, : 2 * HEAD_DIM] / mixed[:, 2 * HEAD_DIM :]
    return jnp.where(low, mixed[:GRID_W], mixed[GRID_W:]).astype(jnp.bfloat16)


MESH = pl.DeviceIdType.MESH
LOG2E = 1.4426950408889634
REACH = NA_ROWS // 2
UP, DOWN = REACH, NA_ROWS - REACH - 1
AHEAD = 4
TALL = 2 * GRID_W


def tp_copy(src, dst, sems, index, peer):
    return pltpu.make_async_remote_copy(
        src_ref=src,
        dst_ref=dst,
        send_sem=sems.at[0, index],
        recv_sem=sems.at[1, index],
        device_id=(lax.axis_index("sp"), peer),
        device_id_type=MESH,
    )


class SquareGather:
    def __init__(self, slots, sems, row_of, halves):
        self.slots, self.sems, self.row_of, self.halves = slots, sems, row_of, halves
        self.me = lax.axis_index("tp")
        self.across = self.me + 1 - 2 * (self.me % 2)
        self.over = (self.me + 2) % 4
        self.corner = (self.across + 2) % 4

    def copy(self, kind, slot, index, half, peer):
        start = pl.multiple_of(self.row_of(index) * GRID_W, GRID_W)
        width = self.slots.shape[2]
        if kind == 2 or self.halves == 2:
            width = width // 2
        cols = slice(half * width, (half + 1) * width)
        part = self.slots.at[slot, pl.ds(start, GRID_W), cols]
        return tp_copy(part, part, self.sems.at[kind], 2 * index + half, peer)

    def send(self, index, half=0):
        self.copy(0, self.me, index, half, self.across).start()
        self.copy(1, self.me, index, half, self.over).start()

    def relay(self, index, half):
        take = half if self.halves == 2 else 0
        if half == 0:
            self.copy(0, self.across, index, take, self.across).wait_recv()
            self.copy(2, self.across, index, half, self.over).start()
        else:
            self.copy(1, self.over, index, take, self.over).wait_recv()
            self.copy(2, self.over, index, half, self.across).start()

    def settle(self, index):
        self.copy(0, self.across, index, 1, self.across).wait_recv()
        self.copy(1, self.over, index, 0, self.over).wait_recv()

    def finish(self, index):
        self.copy(2, self.corner, index, 0, self.over).wait_recv()
        self.copy(2, self.corner, index, 1, self.across).wait_recv()

    def drain(self, index):
        for half in range(self.halves):
            self.copy(0, self.me, index, half, self.across).wait_send()
            self.copy(1, self.me, index, half, self.over).wait_send()
        self.copy(2, self.across, index, 0, self.over).wait_send()
        self.copy(2, self.over, index, 1, self.across).wait_send()


def halo_needs(rows_dev, sp_size):
    rows_all = rows_dev * sp_size
    picks = {"first": 0, "last": sp_size - 1}
    if sp_size > 2:
        picks.update(even=2, odd=1)
    needs = {}
    for kind, sp in picks.items():
        base, seen, steps = sp * rows_dev, set(), []
        for index in range(rows_dev):
            row = base + (index if sp % 2 else rows_dev - 1 - index)
            start = min(max(row - REACH, 0), rows_all - NA_ROWS)
            window = range(start, start + NA_ROWS)
            new = [(True, k) for k in range(UP) if base - UP + k in window]
            new += [(False, k) for k in range(DOWN) if base + rows_dev + k in window]
            steps.append([need for need in new if need not in seen])
            seen.update(new)
        for k in range(UP):
            if sp > 0 and (True, k) not in seen:
                steps[-1].append((True, k))
        for k in range(DOWN):
            if sp < sp_size - 1 and (False, k) not in seen:
                steps[-1].append((False, k))
        needs[kind] = steps
    return needs


def stack_kernel(
    rows_dev, needs,
    x_ref, gain_ref, bias_ref, wq_ref, wk_ref, wv_ref, wo_ref, out_ref,
    gains, weights, stream, mixed, keyval, queries, scaled, squares, own_squares, sums, parts, tables, bias, partial,
    weight_sems, gain_sems, stream_sems, mixed_sems, halo_sems, local_sems,
):
    sp, sp_size = lax.axis_index("sp"), lax.axis_size("sp")
    layers = wq_ref.shape[0]
    tokens, feats = x_ref.shape
    width, total_feats = feats, 4 * feats
    even = 1 - sp % 2

    def row_of(index):
        return index + even * (rows_dev - 1 - 2 * index)

    streams = SquareGather(stream, stream_sems, row_of, 1)
    mixes = SquareGather(mixed, mixed_sems, row_of, 2)
    me, across, over, corner = streams.me, streams.across, streams.over, streams.corner
    sources = (wk_ref, wv_ref, wq_ref, wo_ref)

    def rows_at(row):
        return pl.ds(pl.multiple_of(row * GRID_W, GRID_W), GRID_W)

    def pair_at(chunk):
        low = jnp.minimum(row_of(2 * chunk), row_of(2 * chunk + 1))
        return pl.ds(pl.multiple_of(low * GRID_W, TALL), TALL)

    def weight_copy(kind, layer):
        return pltpu.make_async_copy(
            sources[kind].at[layer], weights.at[kind, layer], weight_sems.at[kind, layer]
        )

    load_x = pltpu.make_async_copy(x_ref, stream.at[me], local_sems.at[rows_dev])
    load_bias = pltpu.make_async_copy(bias_ref, bias, local_sems.at[rows_dev + 1])
    load_x.start()
    load_bias.start()

    barrier = pltpu.get_barrier_semaphore()
    for peer in (across, over, corner):
        pl.semaphore_signal(barrier, inc=1, device_id=(sp, peer), device_id_type=MESH)

    @pl.when(sp > 0)
    def _():
        pl.semaphore_signal(barrier, inc=1, device_id=(sp - 1, me), device_id_type=MESH)

    @pl.when(sp < sp_size - 1)
    def _():
        pl.semaphore_signal(barrier, inc=1, device_id=(sp + 1, me), device_id_type=MESH)

    for layer in range(layers):
        for kind in range(4):
            weight_copy(kind, layer).start()

    gains[me, 0:layers, :] = gain_ref[...].astype(jnp.float32)
    sides = jnp.minimum(sp, 1) + jnp.minimum(sp_size - 1 - sp, 1)
    load_x.wait()
    pl.semaphore_wait(barrier, 3 + sides)

    def gain_copy(index, slot, peer):
        return tp_copy(gains.at[slot], gains.at[slot], gain_sems, index, peer)

    for index, peer in enumerate((across, over, corner)):
        gain_copy(index, me, peer).start()
    for index in range(AHEAD):
        streams.send(index)

    def halo_copy(parity, up, k):
        local = rows_dev - UP + k if up else k
        there = k if up else UP + rows_dev + k
        return pltpu.make_async_remote_copy(
            src_ref=keyval.at[parity, rows_at(UP + local), :],
            dst_ref=keyval.at[parity, rows_at(there), :],
            send_sem=halo_sems.at[0, parity, int(up), k],
            recv_sem=halo_sems.at[1, parity, int(up), k],
            device_id=(sp + 1 if up else sp - 1, me),
            device_id_type=MESH,
        )

    def project(layer, slot, kind, source):
        cols = pl.ds(pl.multiple_of(slot * width, width), width)
        return contract(source, weights[kind, layer, :, cols])

    def scale_slot(layer, slot, here):
        part = stream[slot, here, :].astype(jnp.float32)
        square = part * part
        folded = square[:, :128]
        for start in range(128, feats, 128):
            folded += square[:, start : start + 128]
        return (part * gains[slot, pl.ds(layer, 1), :]).astype(jnp.bfloat16), folded

    def drain_mixed(row):
        if row >= DOWN:
            last = rows_dev if row == rows_dev - 1 else row - DOWN + 1
            for done in range(row - DOWN, last):
                mixes.drain(done)

    def relay_stream(layer, index):
        if index == 0:

            @pl.when(layer == 0)
            def _():
                for place, peer in enumerate((across, over, corner)):
                    gain_copy(place, peer, peer).wait_recv()
                    gain_copy(place, me, peer).wait_send()

        streams.relay(index, 0)
        streams.relay(index, 1)
        if index + AHEAD < rows_dev:

            @pl.when(layer == 0)
            def _():
                streams.send(index + AHEAD)

    def own_rows(layer):
        source, folded = scale_slot(layer, me, slice(None))
        for kind in range(3):
            weight_copy(kind, layer).wait()
            whole = project(layer, me, kind, source)
            for chunk in range(rows_dev // 2):
                sums[chunk, kind] = whole[chunk * TALL : (chunk + 1) * TALL]
        for chunk in range(rows_dev // 2):
            own_squares[chunk] = folded[chunk * TALL : (chunk + 1) * TALL]

    def place_of(chunk):
        return chunk + even * (rows_dev // 2 - 1 - 2 * chunk)

    def start_rows(layer, chunk, kind):
        here, place = pair_at(chunk), place_of(chunk)
        slots = (across, over)
        if kind == 0:
            folded = jnp.zeros((TALL, 128), jnp.float32)
            for turn, slot in enumerate(slots):
                scaled[chunk, turn], square = scale_slot(layer, slot, here)
                folded += square
            squares[chunk] = folded
        parts[chunk, kind] = sum(
            project(layer, slot, kind, scaled[chunk, turn]) for turn, slot in enumerate(slots)
        )

    def end_rows(layer, chunk, part):
        here, place, parity = pair_at(chunk), place_of(chunk), layer % 2
        if part == 1:
            queries[here, :] = (
                (sums[place, 2] + parts[chunk, 2] + project(layer, corner, 2, scaled[chunk, 2]))
                * (squares[chunk, :, :1] * (HEAD_DIM ** (-0.5) * LOG2E))
            ).astype(jnp.bfloat16)
            return
        rows = (2 * chunk, 2 * chunk + 1)
        for index in rows:
            streams.finish(index)
        source, folded = scale_slot(layer, corner, here)
        scaled[chunk, 2] = source
        total = jnp.sum(own_squares[place] + squares[chunk] + folded, axis=1, keepdims=True)
        inverse = lax.rsqrt(total * (1.0 / total_feats) + epsilon)
        squares[chunk] = jnp.broadcast_to(inverse, (TALL, 128))
        there = pl.ds(pl.multiple_of(here.start + UP * GRID_W, GRID_W), TALL)
        for kind in range(2):
            keyval[parity, there, kind * width : (kind + 1) * width] = (
                (sums[place, kind] + parts[chunk, kind] + project(layer, corner, kind, source))
                * inverse
            ).astype(jnp.bfloat16)
        for index in rows:
            row = row_of(index)

            @pl.when((row < DOWN) & (sp > 0))
            def _(row=row):
                halo_copy(parity, False, row).start()

            @pl.when((row >= rows_dev - UP) & (sp < sp_size - 1))
            def _(row=row):
                halo_copy(parity, True, row - (rows_dev - UP)).start()

    def next_tables(layer):
        pl.when(layer < layers - 1)(lambda: make_tables(layer + 1))

    def make_tables(layer):
        low, high = pair_lanes(bias[layer])
        heads = bias.shape[2]

        def lanes_of(pair):
            def at(off):
                place = off * heads + 2 * pair
                return low[place : place + 1] + high[place + 1 : place + 2]

            return at

        for pair in range(width // 128):
            build_table(lanes_of(pair), tables.at[pair])

    kinds = {
        "first": sp == 0,
        "last": sp == sp_size - 1,
        "even": (even == 1) & (sp > 0),
        "odd": (even == 0) & (sp < sp_size - 1),
    }
    early = kinds["odd"]

    def wait_halo(parity, index):
        for kind, steps in needs.items():
            if steps[index]:

                @pl.when(kinds[kind])
                def _(rows=steps[index]):
                    for up, k in rows:
                        halo_copy(parity, up, k).wait_recv()

    def attend(layer, index, half):
        row, parity = row_of(index), layer % 2
        here = rows_at(row)
        if half == 0:
            wait_halo(parity, index)
        base = sp * rows_dev
        first = jnp.clip(base + row - REACH, 0, rows_dev * sp_size - NA_ROWS)
        start, off = first - base + UP, first - base - row + NA_ROWS - 1
        keys = pl.ds(pl.multiple_of(start * GRID_W, GRID_W), NA_ROWS * GRID_W)
        offs = pl.ds(pl.multiple_of(off * GRID_W, GRID_W), NA_ROWS * GRID_W)
        pairs = width // 256
        for pair in range(half * pairs, (half + 1) * pairs):
            cols = slice(pair * 128, (pair + 1) * 128)
            vcols = slice(width + pair * 128, width + (pair + 1) * 128)
            mixed[me, here, cols] = attend_row(
                queries[here, cols],
                keyval[parity, keys, cols],
                keyval[parity, keys, vcols],
                tables[pair, offs, :],
            )
        if half == 1:
            streams.drain(index)
        mixes.send(index, half)
        if index == rows_dev - 1 and half == 1:

            @pl.when(sp > 0)
            def _():
                for k in range(DOWN):
                    halo_copy(parity, False, k).wait_send()

            @pl.when(sp < sp_size - 1)
            def _():
                for k in range(UP):
                    halo_copy(parity, True, k).wait_send()

    def relay_mixed(layer, index, half):
        mixes.relay(index, half)

    def start_mixed(layer, chunk):
        here = pair_at(chunk)
        for index in (2 * chunk, 2 * chunk + 1):
            mixes.settle(index)
        if chunk == 0:
            weight_copy(3, layer).wait()
        total = stream[me, here, :].astype(jnp.float32)
        for slot in (me, across, over):
            total += project(layer, slot, 3, mixed[slot, here, :])
        partial[chunk] = total

    def store_out(chunk):
        here = pair_at(chunk)
        return pltpu.make_async_copy(
            stream.at[me, here, :], out_ref.at[here, :], local_sems.at[chunk]
        )

    def end_mixed(layer, chunk):
        here = pair_at(chunk)
        rows = (2 * chunk, 2 * chunk + 1)
        for index in rows:
            mixes.finish(index)
        total = partial[chunk] + project(layer, corner, 3, mixed[corner, here, :])
        stream[me, here, :] = total.astype(jnp.bfloat16)

        @pl.when(layer < layers - 1)
        def _():
            for index in rows:
                drain_mixed(index)
                streams.send(index)

        @pl.when(layer == layers - 1)
        def _():
            store_out(chunk).start()

    plan = (
        (own_rows, None),
        (relay_stream, None, 0),
        (relay_stream, None, 1),
        (start_rows, None, 0, 0),
        (start_rows, None, 0, 1),
        (start_rows, None, 0, 2),
        (relay_stream, None, 2),
        (relay_stream, None, 3),
        (start_rows, None, 1, 0),
        (start_rows, None, 1, 1),
        (start_rows, None, 1, 2),
        (relay_stream, None, 4),
        (relay_stream, None, 5),
        (start_rows, None, 2, 0),
        (start_rows, None, 2, 1),
        (end_rows, None, 0, 0),
        (end_rows, None, 1, 0),
        (end_rows, None, 2, 0),
        (end_rows, None, 0, 1),
        (start_rows, None, 2, 2),
        (end_rows, None, 2, 1),
        (end_rows, None, 1, 1),
        (attend, None, 0, 0),
        (attend, None, 0, 1),
        (attend, None, 1, 0),
        (attend, None, 1, 1),
        (attend, None, 2, 0),
        (attend, ~early, 2, 1),
        (attend, ~early, 3, 0),
        (attend, ~early, 3, 1),
        (attend, ~early, 4, 0),
        (attend, ~early, 4, 1),
        (attend, ~early, 5, 0),
        (attend, ~early, 5, 1),
        (relay_mixed, None, 0, 0),
        (relay_mixed, None, 0, 1),
        (relay_mixed, None, 1, 0),
        (attend, early, 2, 1),
        (attend, early, 3, 0),
        (attend, early, 3, 1),
        (attend, early, 4, 0),
        (attend, early, 4, 1),
        (attend, early, 5, 0),
        (attend, early, 5, 1),
        (relay_mixed, None, 1, 1),
        (start_mixed, None, 0),
        (relay_mixed, None, 2, 0),
        (relay_mixed, None, 2, 1),
        (relay_mixed, None, 3, 0),
        (relay_mixed, None, 3, 1),
        (start_mixed, None, 1),
        (relay_mixed, None, 4, 0),
        (relay_mixed, None, 4, 1),
        (relay_mixed, None, 5, 0),
        (relay_mixed, None, 5, 1),
        (start_mixed, None, 2),
        (end_mixed, None, 0),
        (next_tables, None),
        (end_mixed, None, 1),
        (end_mixed, None, 2),
    )

    def one_layer(layer, carry):
        for step, when, *place in plan:
            if when is None:
                step(layer, *place)
            else:
                pl.when(when)(lambda: step(layer, *place))
        return carry

    load_bias.wait()
    make_tables(0)
    lax.fori_loop(0, layers, one_layer, 0)
    for index in range(rows_dev):
        mixes.drain(index)
    for chunk in range(rows_dev // 2):
        store_out(chunk).wait()


def square_device(residual, norm_gain, w_query, w_key, w_value, w_out, offset_bias):
    tokens, feats = residual.shape
    layers, heads, row_offs, col_offs = offset_bias.shape
    rows_dev = tokens // GRID_W
    vmem = pl.BlockSpec(memory_space=pltpu.VMEM)
    hbm = pl.BlockSpec(memory_space=pl.ANY)
    bf16, f32, dma = jnp.bfloat16, jnp.float32, pltpu.SemaphoreType.DMA
    padded = tokens + (UP + DOWN) * GRID_W
    needs = halo_needs(rows_dev, lax.axis_size("sp"))
    return pl.pallas_call(
        lambda *refs: stack_kernel(rows_dev, needs, *refs),
        out_shape=jax.ShapeDtypeStruct(residual.shape, bf16),
        in_specs=[hbm, vmem] + [hbm] * 5,
        out_specs=hbm,
        scratch_shapes=[
            pltpu.VMEM((4, -(-layers // 8) * 8, feats), f32),
            pltpu.VMEM((4,) + w_query.shape, bf16),
            pltpu.VMEM((4, tokens, feats), bf16),
            pltpu.VMEM((4, tokens, feats), bf16),
            pltpu.VMEM((2, padded, 2 * feats), bf16),
            pltpu.VMEM((tokens, feats), bf16),
            pltpu.VMEM((rows_dev // 2, 3, TALL, feats), bf16),
            pltpu.VMEM((rows_dev // 2, TALL, 128), f32),
            pltpu.VMEM((rows_dev // 2, TALL, 128), f32),
            pltpu.VMEM((rows_dev // 2, 3, TALL, feats), f32),
            pltpu.VMEM((rows_dev // 2, 3, TALL, feats), f32),
            pltpu.VMEM((feats // 128, row_offs * GRID_W, 128), f32),
            pltpu.VMEM((layers, row_offs, heads, col_offs), f32),
            pltpu.VMEM((rows_dev // 2, TALL, feats), f32),
            dma((4, layers)),
            dma((2, 3)),
            dma((3, 2, 2 * rows_dev)),
            dma((3, 2, 2 * rows_dev)),
            dma((2, 2, 2, max(UP, DOWN))),
            dma((rows_dev + 2,)),
        ],
        compiler_params=pltpu.CompilerParams(
            collective_id=0, has_side_effects=True, vmem_limit_bytes=56 * 1024 * 1024
        ),
        name="stack",
    )(residual, norm_gain, offset_bias.transpose(0, 2, 1, 3), w_query, w_key, w_value, w_out)


def per_device(residual, norm_gain, w_query, w_key, w_value, w_out, offset_bias):
    paired = offset_bias.shape[1] % 8 == 0 and 2 * HEAD_DIM == 128 and 2 * GRID_W == 128
    square = lax.axis_size("tp") == 4 and offset_bias.shape[1] * HEAD_DIM == residual.shape[1]
    rows_dev = residual.shape[0] // GRID_W
    even = lax.axis_size("sp") % 2 == 0 and rows_dev == 2 * (AHEAD - 1)
    body = generic_device
    if paired and square and even:
        body = square_device
    return body(residual, norm_gain, w_query, w_key, w_value, w_out, offset_bias)


def solution(mesh):
    in_specs = (
        P("sp", "tp"),
        P(None, "tp"),
        P(None, "tp", None),
        P(None, "tp", None),
        P(None, "tp", None),
        P(None, "tp", None),
        P(None, "tp", None, None),
    )
    out_specs = P("sp", "tp")
    return jax.shard_map(
        per_device, mesh=mesh, in_specs=in_specs, out_specs=out_specs, check_vma=False
    )
```

```python
import jax
import jax.numpy as jnp
from jax import lax
from jax.experimental import pallas as pl
from jax.experimental.pallas import tpu as pltpu
from jax.sharding import PartitionSpec as P

HEAD_DIM = 64
GRID_W = 64
NA_ROWS = 8
NA_COLS = 16
LAYERS = 3


epsilon = 1e-06


def padded_2(array, sides, width):
    for axis, dim in sides:
        size, length = (lax.axis_size(axis), array.shape[dim])
        up = [(i, (i + 1) % size) for i in range(size - 1)]
        down = [(j, i) for i, j in up]
        last = lax.slice_in_dim(array, length - width, length, axis=dim)
        first = lax.slice_in_dim(array, 0, width, axis=dim)
        before = lax.ppermute(last, axis, up)
        after = lax.ppermute(first, axis, down)
        array = jnp.concatenate([before, array, after], axis=dim)
    return array


def shortened(array):
    return jax.tree.map(lambda a: a.astype(jnp.bfloat16) if a.dtype == jnp.float32 else a, array)


def contract(left, right):
    return lax.dot_general(
        left, right, (((1,), (1,)), ((), ())), preferred_element_type=jnp.float32
    )


def generic_device(residual, norm_gain, w_query, w_key, w_value, w_out, offset_bias):
    token_count = residual.shape[0]
    local_feats = residual.shape[1]
    local_heads = offset_bias.shape[1]
    head_cols = local_heads * HEAD_DIM
    rows_dev = token_count // GRID_W
    rows_all = rows_dev * lax.axis_size("sp")
    row_base = lax.axis_index("sp") * rows_dev
    reach = NA_ROWS // 2
    slab_width = min(2 * NA_COLS, GRID_W)
    tile_starts = list(range(0, GRID_W, NA_COLS))
    slab_starts = [min(max(start - NA_COLS // 2, 0), GRID_W - slab_width) for start in tile_starts]
    tile_info = []
    for start, slab in zip(tile_starts, slab_starts):
        query_cols = start + jnp.arange(NA_COLS, dtype=jnp.int32)
        key_cols = slab + jnp.arange(slab_width, dtype=jnp.int32)
        first_col = jnp.clip(query_cols - NA_COLS // 2, 0, GRID_W - NA_COLS)
        inside = (key_cols[None, :] >= first_col[:, None]) & (
            key_cols[None, :] < first_col[:, None] + NA_COLS
        )
        offsets = key_cols[None, :] - query_cols[:, None] + (NA_COLS - 1)
        onehot = (offsets[:, :, None] == jnp.arange(2 * NA_COLS - 1, dtype=jnp.int32)).astype(
            jnp.float32
        )
        tile_info.append((start, slab, inside, onehot))
    stream = residual
    for layer_index in range(LAYERS):
        res_float = stream.astype(jnp.float32)
        gathered, gain_all = (
            lax.all_gather(stream, "tp", axis=1, tiled=True),
            lax.all_gather(norm_gain[layer_index][None, :], "tp", axis=1, tiled=True),
        )
        full_float = gathered.astype(jnp.float32)
        inverse = lax.rsqrt(jnp.mean(full_float * full_float, axis=1, keepdims=True) + epsilon)
        normed_all = (full_float * inverse * gain_all.astype(jnp.float32)).astype(jnp.bfloat16)
        queries = contract(normed_all, w_query[layer_index])
        keys = contract(normed_all, w_key[layer_index])
        values = contract(normed_all, w_value[layer_index])
        queries = queries.astype(jnp.bfloat16)
        key_value = jnp.concatenate(
            [keys.astype(jnp.bfloat16), values.astype(jnp.bfloat16)], axis=1
        )
        padded = padded_2(key_value, (("sp", 0),), reach * GRID_W)
        key_grid = padded.reshape(rows_dev + 2 * reach, GRID_W, 2, local_heads, HEAD_DIM)
        query_grid = queries.reshape(rows_dev, GRID_W, local_heads, HEAD_DIM)
        lookup = offset_bias[layer_index]

        def one_row(row_index, query_row):
            row_global = row_base + row_index
            first_row = jnp.clip(row_global - reach, 0, rows_all - NA_ROWS)
            local_first = first_row - row_base + reach
            window = lax.dynamic_slice_in_dim(key_grid, local_first, NA_ROWS, 0)
            row_offset = (
                first_row + jnp.arange(NA_ROWS, dtype=jnp.int32) - row_global + (NA_ROWS - 1)
            )
            row_onehot = (
                row_offset[:, None] == jnp.arange(2 * NA_ROWS - 1, dtype=jnp.int32)
            ).astype(jnp.float32)
            row_bias = jnp.einsum(
                "hab,ra->hrb", lookup, row_onehot, precision=lax.Precision.HIGHEST
            )
            pieces = []
            for start, slab, inside, onehot in tile_info:
                query_tile = query_row[start : start + NA_COLS]
                slab_keys = window[:, slab : slab + slab_width, 0]
                slab_values = window[:, slab : slab + slab_width, 1]
                bias_terms = jnp.einsum(
                    "hrb,wsb->hwrs", row_bias, onehot, precision=lax.Precision.HIGHEST
                )
                scores = jnp.einsum(
                    "whd,rshd->hwrs", query_tile, slab_keys, preferred_element_type=jnp.float32
                )
                scores = scores * HEAD_DIM ** (-0.5) + bias_terms
                scores = jnp.where(inside[None, :, None, :], scores, -jnp.inf)
                weights = jax.nn.softmax(
                    scores.reshape(local_heads, NA_COLS, NA_ROWS * slab_width), axis=-1
                ).astype(jnp.bfloat16)
                weights = weights.reshape(local_heads, NA_COLS, NA_ROWS, slab_width)
                attended = jnp.einsum(
                    "hwrs,rshd->whd", weights, slab_values, preferred_element_type=jnp.float32
                )
                pieces.append(attended.astype(jnp.bfloat16).reshape(NA_COLS, head_cols))
            return jnp.concatenate(pieces, axis=0)

        attended = jax.vmap(one_row)(jnp.arange(rows_dev, dtype=jnp.int32), query_grid).reshape(
            token_count, head_cols
        )
        portion = jax.tree.map(
            lambda part: lax.all_gather(part, "tp", axis=1, tiled=True), shortened(attended)
        )
        out_rows = lax.slice_in_dim(w_out[layer_index], 0, portion.shape[1], axis=1)
        mixed = jnp.zeros((token_count, local_feats), jnp.float32) + contract(portion, out_rows)
        stream = (res_float + mixed).astype(jnp.bfloat16)
    return stream


def window_mask():
    shape = (GRID_W, 2 * GRID_W)
    key_col = lax.broadcasted_iota(jnp.int32, shape, 0)
    query_col = lax.broadcasted_iota(jnp.int32, shape, 1) % GRID_W
    first = jnp.clip(query_col - NA_COLS // 2, 0, GRID_W - NA_COLS)
    return (key_col >= first) & (key_col < first + NA_COLS)


def flip_matrix(count, base):
    shape = (count, 2 * GRID_W)
    source = lax.broadcasted_iota(jnp.int32, shape, 0)
    lane = lax.broadcasted_iota(jnp.int32, shape, 1)
    return (lane == base + count - 1 - source).astype(jnp.float32)


def pair_lanes(bias):
    row_offs, heads, col_offs = bias.shape
    flat = bias.reshape(row_offs * heads, col_offs)
    low, high = (
        jnp.dot(
            flat,
            flip_matrix(col_offs, base),
            precision=lax.Precision.HIGHEST,
            preferred_element_type=jnp.float32,
        )
        for base in (0, GRID_W)
    )
    return low, high


def build_table(lanes_of, table):
    inside = window_mask()
    for off in range(2 * NA_ROWS - 1):
        row = jnp.broadcast_to(lanes_of(off), (GRID_W, 2 * GRID_W))
        rolled = pltpu.roll(row, 2 * GRID_W - (NA_COLS - 1), axis=1, stride=1, stride_axis=0)
        table[off * GRID_W : (off + 1) * GRID_W, :] = jnp.where(inside, rolled * LOG2E, -1e30)


def attend_row(query, window_keys, window_values, bias):
    low = lax.broadcasted_iota(jnp.int32, query.shape, 1) < HEAD_DIM
    zero = jnp.zeros_like(query)
    block = jnp.concatenate([jnp.where(low, query, zero), jnp.where(low, zero, query)], axis=0)
    scores = contract(window_keys, block) + bias
    weights = jnp.exp2(scores - jnp.max(scores, axis=0, keepdims=True)).astype(jnp.bfloat16)
    ones = jnp.ones_like(window_values)
    mixed = lax.dot_general(
        weights, jnp.concatenate([window_values, ones], axis=1), (((0,), (0,)), ((), ())),
        preferred_element_type=jnp.float32,
    )
    mixed = mixed[:, : 2 * HEAD_DIM] / mixed[:, 2 * HEAD_DIM :]
    return jnp.where(low, mixed[:GRID_W], mixed[GRID_W:]).astype(jnp.bfloat16)


MESH = pl.DeviceIdType.MESH
LOG2E = 1.4426950408889634
REACH = NA_ROWS // 2
UP, DOWN = REACH, NA_ROWS - REACH - 1
AHEAD = 4
TALL = 2 * GRID_W


def tp_copy(src, dst, sems, index, peer):
    return pltpu.make_async_remote_copy(
        src_ref=src,
        dst_ref=dst,
        send_sem=sems.at[0, index],
        recv_sem=sems.at[1, index],
        device_id=(lax.axis_index("sp"), peer),
        device_id_type=MESH,
    )


class SquareGather:
    def __init__(self, slots, sems, row_of, halves):
        self.slots, self.sems, self.row_of, self.halves = slots, sems, row_of, halves
        self.me = lax.axis_index("tp")
        self.across = self.me + 1 - 2 * (self.me % 2)
        self.over = (self.me + 2) % 4
        self.corner = (self.across + 2) % 4

    def copy(self, kind, slot, index, half, peer):
        start = pl.multiple_of(self.row_of(index) * GRID_W, GRID_W)
        width = self.slots.shape[2]
        if kind == 2 or self.halves == 2:
            width = width // 2
        cols = slice(half * width, (half + 1) * width)
        part = self.slots.at[slot, pl.ds(start, GRID_W), cols]
        return tp_copy(part, part, self.sems.at[kind], 2 * index + half, peer)

    def send(self, index, half=0):
        self.copy(0, self.me, index, half, self.across).start()
        self.copy(1, self.me, index, half, self.over).start()

    def relay(self, index, half):
        take = half if self.halves == 2 else 0
        if half == 0:
            self.copy(0, self.across, index, take, self.across).wait_recv()
            self.copy(2, self.across, index, half, self.over).start()
        else:
            self.copy(1, self.over, index, take, self.over).wait_recv()
            self.copy(2, self.over, index, half, self.across).start()

    def settle(self, index):
        self.copy(0, self.across, index, 1, self.across).wait_recv()
        self.copy(1, self.over, index, 0, self.over).wait_recv()

    def finish(self, index):
        self.copy(2, self.corner, index, 0, self.over).wait_recv()
        self.copy(2, self.corner, index, 1, self.across).wait_recv()

    def drain(self, index):
        for half in range(self.halves):
            self.copy(0, self.me, index, half, self.across).wait_send()
            self.copy(1, self.me, index, half, self.over).wait_send()
        self.copy(2, self.across, index, 0, self.over).wait_send()
        self.copy(2, self.over, index, 1, self.across).wait_send()


def halo_needs(rows_dev, sp_size):
    rows_all = rows_dev * sp_size
    picks = {"first": 0, "last": sp_size - 1}
    if sp_size > 2:
        picks.update(even=2, odd=1)
    needs = {}
    for kind, sp in picks.items():
        base, seen, steps = sp * rows_dev, set(), []
        for index in range(rows_dev):
            row = base + (index if sp % 2 else rows_dev - 1 - index)
            start = min(max(row - REACH, 0), rows_all - NA_ROWS)
            window = range(start, start + NA_ROWS)
            new = [(True, k) for k in range(UP) if base - UP + k in window]
            new += [(False, k) for k in range(DOWN) if base + rows_dev + k in window]
            steps.append([need for need in new if need not in seen])
            seen.update(new)
        for k in range(UP):
            if sp > 0 and (True, k) not in seen:
                steps[-1].append((True, k))
        for k in range(DOWN):
            if sp < sp_size - 1 and (False, k) not in seen:
                steps[-1].append((False, k))
        needs[kind] = steps
    return needs


def stack_kernel(
    rows_dev, needs,
    x_ref, gain_ref, bias_ref, wq_ref, wk_ref, wv_ref, wo_ref, out_ref,
    gains, weights, stream, mixed, keyval, queries, scaled, squares, own_squares, sums, parts, tables, bias, own_gain, partial,
    weight_sems, gain_sems, stream_sems, mixed_sems, halo_sems, local_sems,
):
    sp, sp_size = lax.axis_index("sp"), lax.axis_size("sp")
    layers = wq_ref.shape[0]
    tokens, feats = x_ref.shape
    width, total_feats = feats, 4 * feats
    even = 1 - sp % 2

    def row_of(index):
        return index + even * (rows_dev - 1 - 2 * index)

    streams = SquareGather(stream, stream_sems, row_of, 1)
    mixes = SquareGather(mixed, mixed_sems, row_of, 2)
    me, across, over, corner = streams.me, streams.across, streams.over, streams.corner
    sources = (wk_ref, wv_ref, wq_ref, wo_ref)

    def rows_at(row):
        return pl.ds(pl.multiple_of(row * GRID_W, GRID_W), GRID_W)

    def pair_at(chunk):
        low = jnp.minimum(row_of(2 * chunk), row_of(2 * chunk + 1))
        return pl.ds(pl.multiple_of(low * GRID_W, TALL), TALL)

    def weight_copy(kind, layer):
        return pltpu.make_async_copy(
            sources[kind].at[layer], weights.at[kind, layer], weight_sems.at[kind, layer]
        )

    load_x = pltpu.make_async_copy(x_ref, stream.at[me], local_sems.at[rows_dev])
    load_bias = pltpu.make_async_copy(bias_ref, bias, local_sems.at[rows_dev + 1])
    load_gain = pltpu.make_async_copy(gain_ref, own_gain, local_sems.at[rows_dev + 2])
    load_x.start()
    load_gain.start()
    load_bias.start()

    barrier = pltpu.get_barrier_semaphore()
    for peer in (across, over, corner):
        pl.semaphore_signal(barrier, inc=1, device_id=(sp, peer), device_id_type=MESH)

    @pl.when(sp > 0)
    def _():
        pl.semaphore_signal(barrier, inc=1, device_id=(sp - 1, me), device_id_type=MESH)

    @pl.when(sp < sp_size - 1)
    def _():
        pl.semaphore_signal(barrier, inc=1, device_id=(sp + 1, me), device_id_type=MESH)

    for layer in range(layers):
        for kind in range(4):
            weight_copy(kind, layer).start()

    load_gain.wait()
    gains[me, 0:layers, :] = own_gain[...].astype(jnp.float32)
    sides = jnp.minimum(sp, 1) + jnp.minimum(sp_size - 1 - sp, 1)
    load_x.wait()
    pl.semaphore_wait(barrier, 3 + sides)

    def gain_copy(index, slot, peer):
        return tp_copy(gains.at[slot], gains.at[slot], gain_sems, index, peer)

    for index in range(AHEAD):
        streams.send(index)
        if index == 0:
            for place, peer in enumerate((across, over, corner)):
                gain_copy(place, me, peer).start()

    def halo_copy(parity, up, k):
        local = rows_dev - UP + k if up else k
        there = k if up else UP + rows_dev + k
        return pltpu.make_async_remote_copy(
            src_ref=keyval.at[parity, rows_at(UP + local), :],
            dst_ref=keyval.at[parity, rows_at(there), :],
            send_sem=halo_sems.at[0, parity, int(up), k],
            recv_sem=halo_sems.at[1, parity, int(up), k],
            device_id=(sp + 1 if up else sp - 1, me),
            device_id_type=MESH,
        )

    def project(layer, slot, kind, source):
        cols = pl.ds(pl.multiple_of(slot * width, width), width)
        return contract(source, weights[kind, layer, :, cols])

    def scale_slot(layer, slot, here):
        part = stream[slot, here, :].astype(jnp.float32)
        square = part * part
        folded = square[:, :128]
        for start in range(128, feats, 128):
            folded += square[:, start : start + 128]
        return (part * gains[slot, pl.ds(layer, 1), :]).astype(jnp.bfloat16), folded

    def drain_mixed(row):
        if row >= DOWN:
            last = rows_dev if row == rows_dev - 1 else row - DOWN + 1
            for done in range(row - DOWN, last):
                mixes.drain(done)

    def relay_stream(layer, index):
        if index == 0:

            @pl.when(layer == 0)
            def _():
                for place, peer in enumerate((across, over, corner)):
                    gain_copy(place, peer, peer).wait_recv()
                    gain_copy(place, me, peer).wait_send()

        streams.relay(index, 0)
        streams.relay(index, 1)
        if index + AHEAD < rows_dev:

            @pl.when(layer == 0)
            def _():
                streams.send(index + AHEAD)

    def own_rows(layer):
        source, folded = scale_slot(layer, me, slice(None))
        for kind in range(3):
            weight_copy(kind, layer).wait()
            whole = project(layer, me, kind, source)
            for chunk in range(rows_dev // 2):
                sums[chunk, kind] = whole[chunk * TALL : (chunk + 1) * TALL]
        for chunk in range(rows_dev // 2):
            own_squares[chunk] = folded[chunk * TALL : (chunk + 1) * TALL]

    def place_of(chunk):
        return chunk + even * (rows_dev // 2 - 1 - 2 * chunk)

    def start_rows(layer, chunk, kind):
        here, place = pair_at(chunk), place_of(chunk)
        slots = (across, over)
        if kind == 0:
            folded = jnp.zeros((TALL, 128), jnp.float32)
            for turn, slot in enumerate(slots):
                scaled[chunk, turn], square = scale_slot(layer, slot, here)
                folded += square
            squares[chunk] = folded
        parts[chunk, kind] = sum(
            project(layer, slot, kind, scaled[chunk, turn]) for turn, slot in enumerate(slots)
        )

    def end_rows(layer, chunk, part):
        here, place, parity = pair_at(chunk), place_of(chunk), layer % 2
        if part == 1:
            queries[here, :] = (
                (sums[place, 2] + parts[chunk, 2] + project(layer, corner, 2, scaled[chunk, 2]))
                * (squares[chunk, :, :1] * (HEAD_DIM ** (-0.5) * LOG2E))
            ).astype(jnp.bfloat16)
            return
        rows = (2 * chunk, 2 * chunk + 1)
        for index in rows:
            streams.finish(index)
        source, folded = scale_slot(layer, corner, here)
        scaled[chunk, 2] = source
        total = jnp.sum(own_squares[place] + squares[chunk] + folded, axis=1, keepdims=True)
        inverse = lax.rsqrt(total * (1.0 / total_feats) + epsilon)
        squares[chunk] = jnp.broadcast_to(inverse, (TALL, 128))
        there = pl.ds(pl.multiple_of(here.start + UP * GRID_W, GRID_W), TALL)
        for kind in range(2):
            keyval[parity, there, kind * width : (kind + 1) * width] = (
                (sums[place, kind] + parts[chunk, kind] + project(layer, corner, kind, source))
                * inverse
            ).astype(jnp.bfloat16)
        for index in rows:
            row = row_of(index)

            @pl.when((row < DOWN) & (sp > 0))
            def _(row=row):
                halo_copy(parity, False, row).start()

            @pl.when((row >= rows_dev - UP) & (sp < sp_size - 1))
            def _(row=row):
                halo_copy(parity, True, row - (rows_dev - UP)).start()

    def next_tables(layer):
        pl.when(layer < layers - 1)(lambda: make_tables(layer + 1))

    def make_tables(layer):
        low, high = pair_lanes(bias[layer])
        heads = bias.shape[2]

        def lanes_of(pair):
            def at(off):
                place = off * heads + 2 * pair
                return low[place : place + 1] + high[place + 1 : place + 2]

            return at

        for pair in range(width // 128):
            build_table(lanes_of(pair), tables.at[pair])

    kinds = {
        "first": sp == 0,
        "last": sp == sp_size - 1,
        "even": (even == 1) & (sp > 0),
        "odd": (even == 0) & (sp < sp_size - 1),
    }
    early = kinds["odd"]

    def wait_halo(parity, index):
        for kind, steps in needs.items():
            if steps[index]:

                @pl.when(kinds[kind])
                def _(rows=steps[index]):
                    for up, k in rows:
                        halo_copy(parity, up, k).wait_recv()

    def attend(layer, index, half):
        row, parity = row_of(index), layer % 2
        here = rows_at(row)
        if half == 0:
            wait_halo(parity, index)
        base = sp * rows_dev
        first = jnp.clip(base + row - REACH, 0, rows_dev * sp_size - NA_ROWS)
        start, off = first - base + UP, first - base - row + NA_ROWS - 1
        keys = pl.ds(pl.multiple_of(start * GRID_W, GRID_W), NA_ROWS * GRID_W)
        offs = pl.ds(pl.multiple_of(off * GRID_W, GRID_W), NA_ROWS * GRID_W)
        pairs = width // 256
        for pair in range(half * pairs, (half + 1) * pairs):
            cols = slice(pair * 128, (pair + 1) * 128)
            vcols = slice(width + pair * 128, width + (pair + 1) * 128)
            mixed[me, here, cols] = attend_row(
                queries[here, cols],
                keyval[parity, keys, cols],
                keyval[parity, keys, vcols],
                tables[pair, offs, :],
            )
        if half == 1:
            streams.drain(index)
        mixes.send(index, half)
        if index == rows_dev - 1 and half == 1:

            @pl.when(sp > 0)
            def _():
                for k in range(DOWN):
                    halo_copy(parity, False, k).wait_send()

            @pl.when(sp < sp_size - 1)
            def _():
                for k in range(UP):
                    halo_copy(parity, True, k).wait_send()

    def relay_mixed(layer, index, half):
        mixes.relay(index, half)
        if index == 0 and half == 0:
            weight_copy(3, layer).wait()

    def start_mixed(layer, chunk):
        here = pair_at(chunk)
        for index in (2 * chunk, 2 * chunk + 1):
            mixes.settle(index)
        total = stream[me, here, :].astype(jnp.float32)
        for slot in (me, across, over):
            total += project(layer, slot, 3, mixed[slot, here, :])
        partial[chunk] = total

    def store_out(chunk):
        here = pair_at(chunk)
        return pltpu.make_async_copy(
            stream.at[me, here, :], out_ref.at[here, :], local_sems.at[chunk]
        )

    def end_mixed(layer, chunk):
        here = pair_at(chunk)
        rows = (2 * chunk, 2 * chunk + 1)
        for index in rows:
            mixes.finish(index)
        total = partial[chunk] + project(layer, corner, 3, mixed[corner, here, :])
        stream[me, here, :] = total.astype(jnp.bfloat16)

        @pl.when(layer < layers - 1)
        def _():
            for index in rows:
                drain_mixed(index)
                streams.send(index)

        @pl.when(layer == layers - 1)
        def _():
            store_out(chunk).start()

    plan = (
        (own_rows, None),
        (relay_stream, None, 0),
        (relay_stream, None, 1),
        (relay_stream, None, 2),
        (start_rows, None, 0, 0),
        (relay_stream, None, 3),
        (start_rows, None, 1, 0),
        (start_rows, None, 1, 1),
        (start_rows, None, 1, 2),
        (start_rows, None, 0, 1),
        (start_rows, None, 0, 2),
        (relay_stream, None, 4),
        (relay_stream, None, 5),
        (end_rows, None, 0, 0),
        (end_rows, None, 1, 0),
        (start_rows, None, 2, 0),
        (start_rows, None, 2, 1),
        (end_rows, None, 2, 0),
        (end_rows, None, 0, 1),
        (end_rows, None, 1, 1),
        (start_rows, None, 2, 2),
        (end_rows, None, 2, 1),
        (attend, None, 0, 0),
        (attend, None, 0, 1),
        (attend, None, 1, 0),
        (attend, None, 1, 1),
        (attend, None, 2, 0),
        (attend, None, 2, 1),
        (attend, ~early, 3, 0),
        (attend, ~early, 3, 1),
        (attend, ~early, 4, 0),
        (attend, ~early, 4, 1),
        (attend, ~early, 5, 0),
        (attend, ~early, 5, 1),
        (relay_mixed, None, 0, 0),
        (relay_mixed, None, 0, 1),
        (relay_mixed, None, 1, 0),
        (relay_mixed, None, 1, 1),
        (relay_mixed, None, 2, 0),
        (attend, early, 3, 0),
        (attend, early, 3, 1),
        (attend, early, 4, 0),
        (attend, early, 4, 1),
        (attend, early, 5, 0),
        (attend, early, 5, 1),
        (relay_mixed, None, 2, 1),
        (relay_mixed, None, 3, 0),
        (relay_mixed, None, 3, 1),
        (start_mixed, None, 1),
        (relay_mixed, None, 4, 0),
        (start_mixed, None, 0),
        (relay_mixed, None, 4, 1),
        (relay_mixed, None, 5, 0),
        (relay_mixed, None, 5, 1),
        (end_mixed, None, 0),
        (start_mixed, None, 2),
        (end_mixed, None, 1),
        (end_mixed, None, 2),
        (next_tables, None),
    )

    def one_layer(layer, carry):
        for step, when, *place in plan:
            if when is None:
                step(layer, *place)
            else:
                pl.when(when)(lambda: step(layer, *place))
        return carry

    load_bias.wait()
    make_tables(0)
    lax.fori_loop(0, layers, one_layer, 0)
    for index in range(rows_dev):
        mixes.drain(index)
    for chunk in range(rows_dev // 2):
        store_out(chunk).wait()


def square_device(residual, norm_gain, w_query, w_key, w_value, w_out, offset_bias):
    tokens, feats = residual.shape
    layers, heads, row_offs, col_offs = offset_bias.shape
    rows_dev = tokens // GRID_W
    hbm = pl.BlockSpec(memory_space=pl.ANY)
    bf16, f32, dma = jnp.bfloat16, jnp.float32, pltpu.SemaphoreType.DMA
    padded = tokens + (UP + DOWN) * GRID_W
    needs = halo_needs(rows_dev, lax.axis_size("sp"))
    return pl.pallas_call(
        lambda *refs: stack_kernel(rows_dev, needs, *refs),
        out_shape=jax.ShapeDtypeStruct(residual.shape, bf16),
        in_specs=[hbm] * 7,
        out_specs=hbm,
        scratch_shapes=[
            pltpu.VMEM((4, -(-layers // 8) * 8, feats), f32),
            pltpu.VMEM((4,) + w_query.shape, bf16),
            pltpu.VMEM((4, tokens, feats), bf16),
            pltpu.VMEM((4, tokens, feats), bf16),
            pltpu.VMEM((2, padded, 2 * feats), bf16),
            pltpu.VMEM((tokens, feats), bf16),
            pltpu.VMEM((rows_dev // 2, 3, TALL, feats), bf16),
            pltpu.VMEM((rows_dev // 2, TALL, 128), f32),
            pltpu.VMEM((rows_dev // 2, TALL, 128), f32),
            pltpu.VMEM((rows_dev // 2, 3, TALL, feats), f32),
            pltpu.VMEM((rows_dev // 2, 3, TALL, feats), f32),
            pltpu.VMEM((feats // 128, row_offs * GRID_W, 128), f32),
            pltpu.VMEM((layers, row_offs, heads, col_offs), f32),
            pltpu.VMEM(norm_gain.shape, bf16),
            pltpu.VMEM((rows_dev // 2, TALL, feats), f32),
            dma((4, layers)),
            dma((2, 3)),
            dma((3, 2, 2 * rows_dev)),
            dma((3, 2, 2 * rows_dev)),
            dma((2, 2, 2, max(UP, DOWN))),
            dma((rows_dev + 3,)),
        ],
        compiler_params=pltpu.CompilerParams(
            collective_id=0, has_side_effects=True, vmem_limit_bytes=56 * 1024 * 1024
        ),
        name="stack",
    )(residual, norm_gain, offset_bias.transpose(0, 2, 1, 3), w_query, w_key, w_value, w_out)


def per_device(residual, norm_gain, w_query, w_key, w_value, w_out, offset_bias):
    paired = offset_bias.shape[1] % 8 == 0 and 2 * HEAD_DIM == 128 and 2 * GRID_W == 128
    square = lax.axis_size("tp") == 4 and offset_bias.shape[1] * HEAD_DIM == residual.shape[1]
    rows_dev = residual.shape[0] // GRID_W
    even = lax.axis_size("sp") % 2 == 0 and rows_dev == 2 * (AHEAD - 1)
    body = generic_device
    if paired and square and even:
        body = square_device
    return body(residual, norm_gain, w_query, w_key, w_value, w_out, offset_bias)


def solution(mesh):
    in_specs = (
        P("sp", "tp"),
        P(None, "tp"),
        P(None, "tp", None),
        P(None, "tp", None),
        P(None, "tp", None),
        P(None, "tp", None),
        P(None, "tp", None, None),
    )
    out_specs = P("sp", "tp")
    return jax.shard_map(
        per_device, mesh=mesh, in_specs=in_specs, out_specs=out_specs, check_vma=False
    )
```
